256 devices in a mesh: sp: 16 (over y, x), tp: 16 (over z, core).
Axes of the slice: x: 4, y: 4, z: 8, core: 2. Of those that a mesh axis runs over, the one named last changes fastest.
Arguments:
- latent: bfloat16 [8192, 4096], P(('sp', 'tp')), may hold values from -6 to 6
- context: bfloat16 [512, 4096], P('sp'), may hold values from -6 to 6
- condition: float32 [4096], replicated, may hold values from -6 to 6
- context_condition: float32 [4096], replicated, may hold values from -6 to 6
- modulation: bfloat16 [3, 4096, 4096], P(None, 'sp', 'tp'), may hold values from -0.09375 to 0.09375
- query_weight: bfloat16 [4096, 4096], P(None, 'tp'), as said below
- key_weight: bfloat16 [4096, 4096], P(None, 'tp'), as said below
- value_weight: bfloat16 [4096, 4096], P(None, 'tp'), may hold values from -0.09375 to 0.09375
- lambdas: float32 [16], P('tp'), may hold values from 0.3 to 0.8
- context_lift: float32 [16], P('tp'), may hold values from 1.5 to 3
- head_gain: float32 [256], replicated, may hold values from 0.1 to 1.9
- output_weight: bfloat16 [4096, 4096], P('tp'), may hold values from -0.09375 to 0.09375
Outputs:
- result: bfloat16 [8192, 4096], P(('sp', 'tp'))
The draws below stay inside these ranges and needn't reach their ends.
Inputs may be any that keep to these rules, and one draw needn't show every extreme that they name: `query_weight`: entries lie within 200 / sqrt(4096) in magnitude. `key_weight`: entries lie within 6 / sqrt(4096) in magnitude.
All inputs are finite; a program needn't handle non-finite values.
Results may differ from the reference program's by a relative error of at most 0.025.
Values may be sent and summed in bfloat16 or wider, within the bound.
A program may use at most 64 MiB of HBM per device.

```python
import math
import jax
import jax.numpy as jnp
from jax import lax

D = 4096
HEADS = 16
HEAD_DIM = 256
GRID_W = 64
CTX = 512
SEQ = 8192


def common_keys(key):
    gaussian = jax.random.normal(jax.random.fold_in(key, 101), (D, HEADS * HEAD_DIM), jnp.float32)
    return jnp.clip(gaussian, -6.0, 6.0) * D ** (-0.5)


def draw_key_weight(key, part):
    return common_keys(key).astype(jnp.bfloat16)


def draw_query_weight(key, part):
    gaussian = jax.random.normal(jax.random.fold_in(key, 202), (D, HEADS * HEAD_DIM), jnp.float32)
    independent = jnp.clip(gaussian, -6.0, 6.0) * D ** (-0.5)
    return independent.astype(jnp.bfloat16)


def steps_of(rng, extent, shards, low, high):
    gain, own = 1.0, jax.random.fold_in(rng, 6)
    for dim, shards_of in shards:
        heights = jnp.exp(jax.random.uniform(jax.random.fold_in(own, dim), (shards_of,), jnp.float32, low / len(shards), high / len(shards)))
        gain = gain * jnp.repeat(heights, extent[dim] // shards_of).reshape([-1 if axis == dim else 1 for axis in range(len(extent))])
    return gain


def scatter_about(own_key, extent, scale, reach, cuts=(), kind=jnp.bfloat16):
    factor_of = steps_of(own_key, extent, cuts, -0.22, 0.18) if cuts else 1.0
    values = jax.random.normal(own_key, extent, jnp.float32) * scale * factor_of
    return jnp.minimum(jnp.maximum(values, -reach), reach).astype(kind)


def setup_inputs(seed: int = 0) -> dict:
    keys = jax.random.split(jax.random.key(seed), 13)
    latent = scatter_about(keys[0], (SEQ, D), 1.0, 6.0, ((0, 256),))
    context = scatter_about(keys[1], (CTX, D), 1.0, 6.0, ((0, 16),))
    condition = scatter_about(keys[2], (D,), 1.0, 6.0, (), jnp.float32)
    context_condition = scatter_about(keys[3], (D,), 1.0, 6.0, (), jnp.float32)
    modulation = scatter_about(keys[4], (3, D, D), D ** -0.5, 0.09375, ((1, 16), (2, 16)))
    query_weight = draw_query_weight(jax.random.fold_in(keys[12], 71), 0)
    key_weight = draw_key_weight(jax.random.fold_in(keys[12], 71), 0)
    value_weight = scatter_about(keys[7], (D, HEADS * HEAD_DIM), D ** -0.5, 0.09375, ((1, 16),))
    lambdas = jnp.clip(0.3 + 0.5 * jax.random.uniform(keys[8], (HEADS,), jnp.float32) ** steps_of(keys[8], (HEADS,), ((0, 16),), -0.2, 0.2), 0.3, 0.8)
    context_lift = jnp.clip(1.5 + 1.5 * jax.random.uniform(keys[9], (HEADS,), jnp.float32) ** steps_of(keys[9], (HEADS,), ((0, 16),), -0.2, 0.2), 1.5, 3.0)
    head_gain = jnp.clip(1.0 + 0.18 * jax.random.normal(keys[10], (HEAD_DIM,), jnp.float32), 0.1, 1.9)
    output_weight = scatter_about(keys[11], (HEADS * HEAD_DIM, D), (HEADS * HEAD_DIM) ** -0.5, 0.09375, ((0, 16),))
    return {"latent": latent, "context": context, "condition": condition, "context_condition": context_condition, "modulation": modulation, "query_weight": query_weight, "key_weight": key_weight, "value_weight": value_weight, "lambdas": lambdas, "context_lift": context_lift, "head_gain": head_gain, "output_weight": output_weight}


ROPE_BASE = 10000.0
EPSILON = 1e-05

def modulate(tokens_in, offset, scaling):
    values = tokens_in.astype(jnp.float32)
    center = lax.optimization_barrier(jnp.mean(values, axis=-1, keepdims=True))
    spread = lax.optimization_barrier(jnp.mean(jnp.square(values - center), axis=-1, keepdims=True))
    normed = (values - center) * lax.rsqrt(spread + EPSILON)
    return (normed * (1.0 + scaling) + offset).astype(jnp.bfloat16)

def rotate(tensor, places):
    number, head_count, head_width = tensor.shape
    quarter = head_width // 4
    eighth = head_width // 8
    inverse = ROPE_BASE ** (-jnp.arange(eighth, dtype=jnp.float32) / eighth)
    grid_row = (places // GRID_W).astype(jnp.float32)
    grid_col = (places % GRID_W).astype(jnp.float32)
    angles = jnp.stack([grid_row[:, None] * inverse, grid_col[:, None] * inverse], axis=1)
    cosine = jnp.cos(angles)[:, None, None, :, :]
    sine_table = jnp.sin(angles)[:, None, None, :, :]
    pieces = tensor.reshape(number, head_count, 2, 2, quarter)
    first_half = pieces[..., :eighth]
    second = pieces[..., eighth:]
    turned = jnp.concatenate([first_half * cosine - second * sine_table, second * cosine + first_half * sine_table], axis=-1)
    return turned.reshape(number, head_count, head_width)

def reference(latent, context, condition, context_condition, modulation, query_weight, key_weight, value_weight, lambdas, context_lift, head_gain, output_weight):
    silu_pair = jax.nn.silu(jnp.stack([condition, context_condition])).astype(jnp.bfloat16)
    mod_vectors = jnp.einsum('cd,rde->cre', silu_pair.astype(jnp.float32), modulation.astype(jnp.float32))
    normed = modulate(latent, mod_vectors[0, 0], mod_vectors[0, 1])
    normed_context = modulate(context, mod_vectors[1, 0], mod_vectors[1, 1])
    seq_len = latent.shape[0]
    half_width = HEAD_DIM // 2
    scale_factor = half_width ** (-0.5)
    query_raw = jnp.dot(normed, query_weight, preferred_element_type=jnp.float32).astype(jnp.bfloat16)
    key_raw = jnp.dot(normed, key_weight, preferred_element_type=jnp.float32).astype(jnp.bfloat16)
    latent_values = jnp.dot(normed, value_weight, preferred_element_type=jnp.float32).astype(jnp.bfloat16)
    context_keys = jnp.dot(normed_context, key_weight, preferred_element_type=jnp.float32).astype(jnp.bfloat16)
    context_values = jnp.dot(normed_context, value_weight, preferred_element_type=jnp.float32).astype(jnp.bfloat16)
    places = jnp.arange(seq_len, dtype=jnp.int32)
    queries = rotate(query_raw.astype(jnp.float32).reshape(seq_len, HEADS, HEAD_DIM), places).astype(jnp.bfloat16)
    latent_keys = rotate(key_raw.astype(jnp.float32).reshape(seq_len, HEADS, HEAD_DIM), places).astype(jnp.bfloat16)
    all_keys = jnp.concatenate([context_keys.reshape(CTX, HEADS, HEAD_DIM), latent_keys], axis=0)
    all_values = jnp.concatenate([context_values.reshape(CTX, HEADS, HEAD_DIM), latent_values.reshape(seq_len, HEADS, HEAD_DIM)], axis=0)
    key_total = CTX + seq_len
    block_len = math.gcd(seq_len, 1024)

    def one_head(inputs):
        head_queries, head_keys, head_values, head_lambda, head_lift = inputs
        lift_row = jnp.where(jnp.arange(key_total) < CTX, head_lift, 0.0)

        def one_block(block_queries):
            outputs = []
            for map_index in range(2):
                low_col = map_index * half_width
                scores = jnp.dot(block_queries[:, low_col:low_col + half_width], head_keys[:, low_col:low_col + half_width].T, preferred_element_type=jnp.float32) * scale_factor + lift_row
                row_peak = lax.optimization_barrier(jnp.max(scores, axis=1, keepdims=True))
                weights = jnp.exp(scores - row_peak)
                row_sums = lax.optimization_barrier(jnp.sum(weights, axis=1, keepdims=True))
                outputs.append(jnp.dot(weights.astype(jnp.bfloat16), head_values, preferred_element_type=jnp.float32) / row_sums)
            difference = outputs[0] - head_lambda * outputs[1]
            scaled = difference * lax.rsqrt(lax.optimization_barrier(jnp.mean(jnp.square(difference), axis=1, keepdims=True)) + EPSILON) * head_gain
            return scaled.astype(jnp.bfloat16)
        blocks = head_queries.reshape(seq_len // block_len, block_len, HEAD_DIM)
        return lax.map(one_block, blocks).reshape(seq_len, HEAD_DIM)
    heads_out = lax.map(one_head, (queries.transpose(1, 0, 2), all_keys.transpose(1, 0, 2), all_values.transpose(1, 0, 2), lambdas, context_lift))
    attended = heads_out.transpose(1, 0, 2).reshape(seq_len, HEADS * HEAD_DIM)
    mixture = jnp.dot(attended, output_weight, preferred_element_type=jnp.float32)
    return (latent.astype(jnp.float32) + mod_vectors[0, 2] * mixture).astype(jnp.bfloat16)
```

```python
import functools
import math

import jax
import jax.numpy as jnp
import numpy as np
from jax import lax
from jax.experimental import pallas as pl
from jax.experimental.pallas import tpu as pltpu
from jax.sharding import Mesh
from jax.sharding import PartitionSpec as P

MESH = pl.DeviceIdType.MESH
F32 = jnp.float32
BF16 = jnp.bfloat16
GRID_W = 64
EPS = 1e-5
NZ = 8
NS = 16
D = 4096
HD = 256
PART = 128
ROWS = 32
LOG2E = math.log2(math.e)
ORDER = (0, 7, 1, 6, 2, 5, 3, 4)
PLACE = {rel: i for i, rel in enumerate(ORDER)}
UNIT = 2 * ROWS
BLOCK = NZ * UNIT
ANY = pl.BlockSpec(memory_space=pl.ANY)
VM = pl.BlockSpec(memory_space=pltpu.VMEM)
SM = pl.BlockSpec(memory_space=pltpu.SMEM)


def position():
    return tuple(lax.axis_index(a) for a in ("y", "x", "z", "c"))


def sp_peer(i):
    y, x, z, c = position()
    peer = lax.rem(y * 4 + x + i, NS)
    return (peer // 4, lax.rem(peer, 4), z, c)


def tp_peer(i):
    y, x, z, c = position()
    peer = lax.rem(z * 2 + c + i, NS)
    return (y, x, peer // 2, lax.rem(peer, 2))


def greet(peers):
    barrier = pltpu.get_barrier_semaphore()
    for peer_of in peers:

        def one(i, carry):
            pl.semaphore_signal(barrier, inc=1, device_id=peer_of(i), device_id_type=MESH)
            return carry

        lax.fori_loop(1, NS, one, 0)


def greeted(peers):
    pl.semaphore_wait(pltpu.get_barrier_semaphore(), (NS - 1) * len(peers))


def send(src, dst, send_sem, recv_sem, to):
    pltpu.make_async_remote_copy(
        src_ref=src, dst_ref=dst, send_sem=send_sem, recv_sem=recv_sem, device_id=to, device_id_type=MESH
    ).start()


def await_bytes(ref, sem):
    pltpu.make_async_copy(ref, ref, sem).wait()


def silu(v):
    return v / (1.0 + jnp.exp(-v))


def modulated(tokens, shift, scale):
    values = tokens.astype(F32)
    center = jnp.mean(values, axis=-1, keepdims=True)
    values = values - center
    spread = jnp.mean(values * values, axis=-1, keepdims=True)
    return (values * lax.rsqrt(spread + EPS) * (1.0 + scale) + shift).astype(BF16)


def turned(raw, cos, sin):
    lane = lax.broadcasted_iota(jnp.int32, raw.shape, 1)
    partner = jnp.where(lax.rem(lane, 64) < 32, pltpu.roll(raw, HD - 32, 1), pltpu.roll(raw, 32, 1))
    return (raw * cos + partner * sin).astype(BF16)


def tables():
    inverse = 10000.0 ** (-np.arange(32, dtype=np.float32) / np.float32(32))
    inverse = inverse.astype(np.float32)
    row = (np.arange(128, dtype=np.float32)[:, None] * inverse).astype(np.float32).astype(np.float64)
    col = row[:GRID_W]
    zr, zc = np.zeros((128, 64)), np.zeros((GRID_W, 64))

    def lanes(first, second):
        return np.tile(np.concatenate([first, second], axis=1), (1, 2)).astype(np.float32)

    both = lambda a, b: np.concatenate([a, b], axis=1)
    return (
        lanes(both(np.cos(row), np.cos(row)), zr),
        lanes(both(-np.sin(row), np.sin(row)), zr),
        lanes(zc, both(np.cos(col), np.cos(col))),
        lanes(zc, both(-np.sin(col), np.sin(col))),
    )


def front(
    latent, context, cond, ctx_cond, modulation, wq, wk, wv, rcos, rsin, ccos, csin,
    q_out, kv_out, ctx_out, mods,
    lat, wq_v, wk_v, wv_v, mod_v, ctx_v, parts, normed,
    load, mod_send, mod_recv, ring_send, ring_recv, pair_send, pair_recv,
):
    y, x, z, c = position()
    sp, tp = y * 4 + x, z * 2 + c
    loads = [
        pltpu.make_async_copy(latent, lat.at[z, c], load.at[0]),
        pltpu.make_async_copy(modulation, mod_v, load.at[1]),
        pltpu.make_async_copy(context, ctx_v, load.at[2]),
        pltpu.make_async_copy(wq, wq_v, load.at[3]),
        pltpu.make_async_copy(wk, wk_v, load.at[4]),
        pltpu.make_async_copy(wv, wv_v, load.at[5]),
    ]
    for copy in loads:
        copy.start()

    def half_of(step, way):
        return (0, 1) if step < 4 else ((0,) if way > 0 else (1,))

    def block(rel):
        return lax.rem(z + rel, NZ)

    def ring_step(step, way, half):
        held = block((-way * (step - 1)) % NZ)
        there = (-way * step) % NZ
        rows = pl.ds(half * 16, 16)
        send(
            lat.at[held, c, rows], lat.at[held, c, rows], ring_send.at[there * 2 + half],
            ring_recv.at[there * 2 + half], (y, x, lax.rem(z + way + NZ, NZ), c),
        )

    def ring_wait(rel, half):
        await_bytes(lat.at[block(rel), c, pl.ds(half * 16, 16)], ring_recv.at[rel * 2 + half])

    def pair_step(rel):
        mine = lat.at[block(rel), c]
        send(mine, mine, pair_send.at[rel], pair_recv.at[rel], (y, x, z, 1 - c))

    def pair_wait(rel):
        await_bytes(lat.at[block(rel), 1 - c], pair_recv.at[rel])

    loads[0].wait()
    greeted((sp_peer, tp_peer))
    for half in (0, 1):
        for way in (1, -1):
            ring_step(1, way, half)
    pair_step(0)

    pick = lax.broadcasted_iota(jnp.int32, (8, PART), 0) == 0
    rows = []
    for j in range(2):
        at = pl.ds(sp * 2 + j, 1)
        rows.append(silu(jnp.where(pick, cond[at, :], ctx_cond[at, :])).astype(BF16))
    loads[1].wait()
    for r in range(3):
        product = jnp.dot(rows[0], mod_v[r, 0:PART], preferred_element_type=F32) + jnp.dot(
            rows[1], mod_v[r, PART : 2 * PART], preferred_element_type=F32
        )
        parts[sp, r : r + 1, :] = product[0:1]
        parts[sp, 3 + r : 4 + r, :] = product[1:2]
    parts[sp, 6:8, :] = jnp.zeros((2, HD), F32)

    def show_part(i, carry):
        send(parts.at[sp], parts.at[sp], mod_send.at[0], mod_recv.at[0], sp_peer(i))
        return carry

    lax.fori_loop(1, NS, show_part, 0)
    await_bytes(parts.at[pl.ds(0, NS - 1)], mod_recv.at[0])
    total = parts[0]
    for i in range(1, NS):
        total = total + parts[i]
    own_cols = pl.ds(pl.multiple_of(tp * HD, HD), HD)
    mods[:, own_cols] = total

    def show_sum(i, carry):
        send(mods.at[:, own_cols], mods.at[:, own_cols], mod_send.at[1], mod_recv.at[1], tp_peer(i))
        return carry

    lax.fori_loop(1, NS, show_sum, 0)

    def forward(step):
        for half in (0, 1):
            for way in (1, -1):
                ring_wait((-way * step) % NZ, half)
                if half in half_of(step + 1, way):
                    ring_step(step + 1, way, half)
        for way in (1, -1):
            pair_step((-way * step) % NZ)

    def norm_rows(load_rows, where, pick_mod):
        shift, scale = mods[pick_mod : pick_mod + 1, :], mods[pick_mod + 1 : pick_mod + 2, :]
        for half in (0, 1):
            normed[where + half * 16 : where + half * 16 + 16, :] = modulated(
                load_rows(pl.ds(half * 16, 16)), shift, scale
            )

    def project(units, with_context):
        count = len(units)
        for i, rel in enumerate(units):
            zz = block(rel)
            for core in (0, 1):
                norm_rows(lambda rows, zz=zz, core=core: lat[zz, core, rows, :], i * UNIT + core * ROWS, 0)
        if with_context:
            norm_rows(lambda rows: ctx_v[rows, :], count * UNIT, 3)
        end = count * UNIT + (ROWS if with_context else 0)
        lhs = normed[0:end, :]
        q_raw = jnp.dot(lhs, wq_v[...], preferred_element_type=F32).astype(BF16)
        k_raw = jnp.dot(lhs, wk_v[...], preferred_element_type=F32).astype(BF16)
        v_raw = jnp.dot(lhs, wv_v[...], preferred_element_type=F32).astype(BF16)
        for i, rel in enumerate(units):
            o = PLACE[rel]
            line = pl.ds(sp * NZ + block(rel), 1)
            cos = rcos[line, :] + ccos[...]
            sin = rsin[line, :] + csin[...]
            part = slice(i * UNIT, (i + 1) * UNIT)
            q = turned(q_raw[part].astype(F32), cos, sin)
            for core in (0, 1):
                q_out[core * HD + o * ROWS : core * HD + (o + 1) * ROWS, :] = q[core * ROWS : (core + 1) * ROWS]
            kv_out[o, :, 0:HD] = turned(k_raw[part].astype(F32), cos, sin)
            kv_out[o, :, HD : 2 * HD] = v_raw[part]
        if with_context:
            ctx_out[:, 0:HD] = k_raw[count * UNIT : end]
            ctx_out[:, HD : 2 * HD] = v_raw[count * UNIT : end]

    forward(1)
    await_bytes(mods.at[:, pl.ds(0, (NS - 1) * HD)], mod_recv.at[1])
    for copy in loads[2:]:
        copy.wait()
    pair_wait(0)
    project([0], True)
    forward(2)
    for rel in (7, 1):
        pair_wait(rel)
    project([7, 1], False)
    forward(3)
    for rel in (6, 2):
        pair_wait(rel)
    project([6, 2], False)
    ring_wait(4, 0)
    ring_wait(4, 1)
    pair_step(4)
    for rel in (5, 3):
        pair_wait(rel)
    project([5, 3], False)
    pair_wait(4)
    project([4], False)

    await_bytes(parts.at[pl.ds(0, NS - 1)], mod_send.at[0])
    await_bytes(mods.at[:, pl.ds(0, (NS - 1) * HD)], mod_send.at[1])
    for i in range(2, 2 * NZ):
        await_bytes(lat.at[0, 0, pl.ds(0, 16)], ring_send.at[i])
    for rel in range(NZ):
        await_bytes(lat.at[0, 0], pair_send.at[rel])


def front_kernel(*refs):
    greet((sp_peer, tp_peer))
    front(*refs)


def run_front(latent, context, cond, ctx_cond, modulation, wq, wk, wv):
    dma = pltpu.SemaphoreType.DMA
    return pl.pallas_call(
        front_kernel,
        out_shape=(
            jax.ShapeDtypeStruct((BLOCK, HD), BF16),
            jax.ShapeDtypeStruct((NZ, UNIT, 2 * HD), BF16),
            jax.ShapeDtypeStruct((ROWS, 2 * HD), BF16),
            jax.ShapeDtypeStruct((8, D), F32),
        ),
        in_specs=[ANY, ANY, VM, VM, ANY, ANY, ANY, ANY, VM, VM, VM, VM],
        out_specs=(VM, VM, VM, VM),
        scratch_shapes=[
            pltpu.VMEM((NZ, 2, ROWS, D), BF16),
            pltpu.VMEM((D, HD), BF16),
            pltpu.VMEM((D, HD), BF16),
            pltpu.VMEM((D, HD), BF16),
            pltpu.VMEM((3, HD, HD), BF16),
            pltpu.VMEM((ROWS, D), BF16),
            pltpu.VMEM((NS, 8, HD), F32),
            pltpu.VMEM((2 * UNIT, D), BF16),
            dma((6,)),
            dma((2,)),
            dma((2,)),
            dma((2 * NZ,)),
            dma((2 * NZ,)),
            dma((NZ,)),
            dma((NZ,)),
        ],
        compiler_params=pltpu.CompilerParams(
            collective_id=0, has_side_effects=True, vmem_limit_bytes=40 * 2**20
        ),
        name="front",
    )(latent, context, cond, ctx_cond, modulation, wq, wk, wv, *[jnp.asarray(t) for t in tables()])


def gather_unit(kv, kv_send, kv_recv):
    y, x, z, c = position()

    def geometry(o):
        swap = lax.rem(o, 2)
        way = 1 - 2 * lax.rem(o // 2, 2)
        first = swap * y + (1 - swap) * x
        second = swap * x + (1 - swap) * y
        return swap, way, first, second

    def step(o, geo, df, dg, tf, tg, kind):
        swap, way, first, second = geo

        def pair(f, g):
            f, g = lax.rem(f + 8, 4), lax.rem(g + 8, 4)
            return swap * f + (1 - swap) * g, swap * g + (1 - swap) * f

        oy, ox = pair(first + df, second + dg)
        ty, tx = pair(first + tf, second + tg)
        rows = pl.ds(pl.multiple_of((oy * 4 + ox) * UNIT, UNIT), UNIT)
        send(kv.at[o, rows], kv.at[o, rows], kv_send.at[0], kv_recv.at[o * 5 + kind], (ty, tx, z, c))

    def wait(o, kind, count):
        await_bytes(kv.at[o, pl.ds(0, count * UNIT)], kv_recv.at[o * 5 + kind])

    def own(o):
        geo = geometry(o)
        way = geo[1]
        step(o, geo, 0, 0, 1, 0, 0)
        step(o, geo, 0, 0, -1, 0, 0)
        step(o, geo, 0, 0, 0, way, 1)
        step(o, geo, 0, 0, 0, -way, 4)

    def stage1(o):
        geo = geometry(o)
        way = geo[1]
        wait(o, 0, 2)
        step(o, geo, -way, 0, way, 0, 1)
        for d in (1, -1):
            step(o, geo, d, 0, 0, way, 2)
            step(o, geo, d, 0, 0, -way, 4)

    def stage2(o):
        geo = geometry(o)
        way = geo[1]
        wait(o, 1, 2)
        step(o, geo, 2, 0, 0, way, 3)
        step(o, geo, 2, 0, 0, -way, 4)
        step(o, geo, 0, -way, 0, way, 4)

    def stage3(o):
        geo = geometry(o)
        way = geo[1]
        wait(o, 2, 2)
        for d in (1, -1):
            step(o, geo, d, -way, 0, way, 4)

    def stage4(o):
        geo = geometry(o)
        way = geo[1]
        wait(o, 3, 1)
        step(o, geo, 2, -way, 0, way, 4)

    def done(o):
        wait(o, 4, 8)

    def all_sent():
        for _ in range(NS - 1):
            await_bytes(kv.at[0, pl.ds(0, NZ * UNIT)], kv_send.at[0])

    return own, (stage1, stage2, stage3, stage4), done, all_sent


def absorb(q, key_part, value_part, lift, peak, sums, acc):
    factor = PART**-0.5 * LOG2E
    values = value_part()
    for m in range(2):
        scores = lax.dot_general(
            q[:, m * PART : (m + 1) * PART], key_part(m), (((1,), (1,)), ((), ())), preferred_element_type=F32
        )
        scores = scores * factor
        if lift is not None:
            scores = scores + lift
        before = peak[m]
        now = jnp.maximum(before, jnp.max(scores, axis=1, keepdims=True))
        fading = jnp.exp2(before - now)
        weights = jnp.exp2(scores - now[:, 0:1])
        sums[m] = sums[m] * fading + jnp.sum(weights, axis=1, keepdims=True)
        acc[m] = acc[m] * fading[:, 0:1] + jnp.dot(
            weights.astype(BF16), values, preferred_element_type=F32
        )
        peak[m] = now


def middle(
    q, kv_own, ctx_own, lift, lam, gain,
    attended,
    kv, ctx, peak, sums, acc,
    load, ctx_send, ctx_recv, kv_send, kv_recv,
):
    y, x, z, c = position()
    sp = y * 4 + x
    loads = [
        pltpu.make_async_copy(kv_own, kv.at[:, pl.ds(pl.multiple_of(sp * UNIT, UNIT), UNIT)], load.at[0]),
        pltpu.make_async_copy(ctx_own, ctx.at[pl.ds(pl.multiple_of(sp * ROWS, ROWS), ROWS)], load.at[1]),
    ]
    for copy in loads:
        copy.start()
    peak[...] = jnp.full(peak.shape, -jnp.inf, F32)
    sums[...] = jnp.zeros(sums.shape, F32)
    acc[...] = jnp.zeros(acc.shape, F32)
    own, stages, done, all_sent = gather_unit(kv, kv_send, kv_recv)
    for copy in loads:
        copy.wait()
    greeted((sp_peer,))

    def show_context(i, carry):
        mine = ctx.at[pl.ds(pl.multiple_of(sp * ROWS, ROWS), ROWS)]
        send(mine, mine, ctx_send.at[0], ctx_recv.at[0], sp_peer(i))
        return carry

    lax.fori_loop(1, NS, show_context, 0)

    def start_own(o, carry):
        own(o)
        return carry

    lax.fori_loop(0, NZ, start_own, 0)
    lift_term = lift[0] * LOG2E

    def tick(t, carry):
        for back, stage in enumerate(stages):
            o = t - back

            @pl.when((o >= 0) & (o < NZ))
            def _():
                stage(o)

        @pl.when(t == 1)
        def _():
            await_bytes(ctx.at[pl.ds(0, (NS - 1) * ROWS)], ctx_recv.at[0])
            absorb(
                q, lambda m: ctx[:, m * PART : (m + 1) * PART], lambda: ctx[:, HD : 2 * HD],
                lift_term, peak, sums, acc,
            )

        o = t - len(stages)

        @pl.when(o >= 0)
        def _():
            done(o)

            def part(i, inner):
                rows = pl.ds(pl.multiple_of(i * 512, 512), 512)
                absorb(
                    q, lambda m: kv[o, rows, m * PART : (m + 1) * PART], lambda: kv[o, rows, HD : 2 * HD],
                    None, peak, sums, acc,
                )
                return inner

            lax.fori_loop(0, 2, part, 0)

        return carry

    lax.fori_loop(0, NZ + len(stages), tick, 0)
    means = [acc[m] / sums[m][:, 0:1] for m in range(2)]
    difference = means[0] - lam[0] * means[1]
    spread = jnp.mean(difference * difference, axis=1, keepdims=True)
    attended[...] = (difference * lax.rsqrt(spread + EPS) * gain[...]).astype(BF16)
    all_sent()
    await_bytes(ctx.at[pl.ds(0, (NS - 1) * ROWS)], ctx_send.at[0])


def middle_kernel(*refs):
    greet((sp_peer,))
    middle(*refs)


def run_middle(q, kv_own, ctx_own, lift, lam, gain):
    dma = pltpu.SemaphoreType.DMA
    return pl.pallas_call(
        middle_kernel,
        out_shape=jax.ShapeDtypeStruct((BLOCK, HD), BF16),
        in_specs=[VM, ANY, ANY, SM, SM, VM],
        out_specs=VM,
        scratch_shapes=[
            pltpu.VMEM((NZ, NS * UNIT, 2 * HD), BF16),
            pltpu.VMEM((NS * ROWS, 2 * HD), BF16),
            pltpu.VMEM((2, BLOCK, 128), F32),
            pltpu.VMEM((2, BLOCK, 128), F32),
            pltpu.VMEM((2, BLOCK, HD), F32),
            dma((2,)),
            dma((1,)),
            dma((1,)),
            dma((1,)),
            dma((5 * NZ,)),
        ],
        compiler_params=pltpu.CompilerParams(
            collective_id=1, has_side_effects=True, vmem_limit_bytes=40 * 2**20
        ),
        name="middle",
    )(q, kv_own, ctx_own, lift, lam, gain)


CHUNKS = 4
WIDE = D // CHUNKS


def back(
    attended, wo, latent, mods,
    result,
    mine, theirs, wo_v, wo_pair, lat_v, part, out_buf, in_buf,
    load, pair_send, pair_recv, out_send, out_recv,
):
    y, x, z, c = position()
    pair = (y, x, z, 1 - c)
    loads = [
        pltpu.make_async_copy(wo, wo_v, load.at[0]),
        pltpu.make_async_copy(attended.at[pl.ds(pl.multiple_of(c * HD, HD), HD)], mine, load.at[1]),
        pltpu.make_async_copy(latent, lat_v, load.at[2]),
    ]
    for copy in loads:
        copy.start()
    greeted((tp_peer,))
    send(attended.at[pl.ds(pl.multiple_of((1 - c) * HD, HD), HD)], theirs, pair_send.at[0], pair_recv.at[0], pair)
    loads[0].wait()
    send(wo_v, wo_pair, pair_send.at[1], pair_recv.at[1], pair)
    loads[1].wait()
    await_bytes(theirs, pair_recv.at[0])
    await_bytes(wo_pair, pair_recv.at[1])

    def long_way(j):
        return 0 if j < 2 else 1

    def slot(way, step, j):
        return (way * 4 + step - 1) * CHUNKS + j

    def hop(way, step, j, add):
        rel = (5 - step) if way == 0 else (3 + step) % NZ
        value = part[j, PLACE[rel]]
        if add:
            value = value + in_buf[slot(way, step - 1, j)].astype(F32)
        s = slot(way, step, j)
        out_buf[s] = value.astype(BF16)
        to = lax.rem(z + (1 if way == 0 else NZ - 1), NZ)
        send(out_buf.at[s], in_buf.at[s], out_send.at[s], out_recv.at[s], (y, x, to, c))

    def hop_wait(way, step, j):
        s = slot(way, step, j)
        await_bytes(in_buf.at[s], out_recv.at[s])

    for j in (0, 2, 1, 3):
        cols = slice(j * WIDE, (j + 1) * WIDE)
        product = jnp.dot(mine[...], wo_v[:, cols], preferred_element_type=F32) + jnp.dot(
            theirs[...], wo_pair[:, cols], preferred_element_type=F32
        )
        part[j] = product.reshape(NZ, ROWS, WIDE)
        hop(long_way(j), 1, j, False)
    for j in (0, 2, 1, 3):
        hop(1 - long_way(j), 2, j, False)
    for step in (1, 2, 3):
        if step > 1:
            for j in (0, 2, 1, 3):
                way = 1 - long_way(j)
                hop_wait(way, step, j)
                hop(way, step + 1, j, True)
        for j in (0, 2, 1, 3):
            way = long_way(j)
            hop_wait(way, step, j)
            hop(way, step + 1, j, True)
    loads[2].wait()
    for j in (0, 2, 1, 3):
        cols = slice(j * WIDE, (j + 1) * WIDE)
        total = part[j, 0]
        for way in (1 - long_way(j), long_way(j)):
            hop_wait(way, 4, j)
            total = total + in_buf[slot(way, 4, j)].astype(F32)
        result[:, cols] = (lat_v[:, cols].astype(F32) + mods[2:3, cols] * total).astype(BF16)
    await_bytes(theirs, pair_send.at[0])
    await_bytes(wo_pair, pair_send.at[1])
    for way in (0, 1):
        for step in (1, 2, 3, 4):
            for j in range(CHUNKS):
                if step > 1 or long_way(j) == way:
                    s = slot(way, step, j)
                    await_bytes(out_buf.at[s], out_send.at[s])


def back_kernel(*refs):
    greet((tp_peer,))
    back(*refs)


def run_back(attended, wo, latent, mods):
    dma = pltpu.SemaphoreType.DMA
    slots = 2 * 4 * CHUNKS
    return pl.pallas_call(
        back_kernel,
        out_shape=jax.ShapeDtypeStruct((ROWS, D), BF16),
        in_specs=[ANY, ANY, ANY, VM],
        out_specs=VM,
        scratch_shapes=[
            pltpu.VMEM((HD, HD), BF16),
            pltpu.VMEM((HD, HD), BF16),
            pltpu.VMEM((HD, D), BF16),
            pltpu.VMEM((HD, D), BF16),
            pltpu.VMEM((ROWS, D), BF16),
            pltpu.VMEM((CHUNKS, NZ, ROWS, WIDE), F32),
            pltpu.VMEM((slots, ROWS, WIDE), BF16),
            pltpu.VMEM((slots, ROWS, WIDE), BF16),
            dma((3,)),
            dma((2,)),
            dma((2,)),
            dma((slots,)),
            dma((slots,)),
        ],
        compiler_params=pltpu.CompilerParams(
            collective_id=2, has_side_effects=True, vmem_limit_bytes=40 * 2**20
        ),
        name="back",
    )(attended, wo, latent, mods)


def shards(
    latent, context, condition, context_condition, modulation,
    query_weight, key_weight, value_weight, lambdas, context_lift, head_gain, output_weight,
):
    q, kv_own, ctx_own, mods = run_front(
        latent, context, condition.reshape(32, 128), context_condition.reshape(32, 128),
        modulation, query_weight, key_weight, value_weight,
    )
    attended = run_middle(q, kv_own, ctx_own, context_lift, lambdas, head_gain.reshape(1, HD))
    return run_back(attended, output_weight, latent, mods)


def solution(mesh):
    split = Mesh(mesh.devices.reshape(4, 4, NZ, 2), ("y", "x", "z", "c"))
    sp, tp = ("y", "x"), ("z", "c")
    return jax.shard_map(
        shards,
        mesh=split,
        in_specs=(
            P(sp + tp, None),
            P(sp, None),
            P(),
            P(),
            P(None, sp, tp),
            P(None, tp),
            P(None, tp),
            P(None, tp),
            P(tp),
            P(tp),
            P(),
            P(tp, None),
        ),
        out_specs=P(sp + tp, None),
        check_vma=False,
    )
```

```python
import functools
import math

import jax
import jax.numpy as jnp
import numpy as np
from jax import lax
from jax.experimental import pallas as pl
from jax.experimental.pallas import tpu as pltpu
from jax.sharding import Mesh
from jax.sharding import PartitionSpec as P

MESH = pl.DeviceIdType.MESH
F32 = jnp.float32
BF16 = jnp.bfloat16
GRID_W = 64
EPS = 1e-5
NZ = 8
NS = 16
D = 4096
HD = 256
PART = 128
ROWS = 32
LOG2E = math.log2(math.e)
ORDER = (0, 7, 1, 6, 2, 5, 3, 4)
PLACE = {rel: i for i, rel in enumerate(ORDER)}
UNIT = 2 * ROWS
BLOCK = NZ * UNIT
ANY = pl.BlockSpec(memory_space=pl.ANY)
VM = pl.BlockSpec(memory_space=pltpu.VMEM)
SM = pl.BlockSpec(memory_space=pltpu.SMEM)


def position():
    return tuple(lax.axis_index(a) for a in ("y", "x", "z", "c"))


def sp_peer(i):
    y, x, z, c = position()
    peer = lax.rem(y * 4 + x + i, NS)
    return (peer // 4, lax.rem(peer, 4), z, c)


def tp_peer(i):
    y, x, z, c = position()
    peer = lax.rem(z * 2 + c + i, NS)
    return (y, x, peer // 2, lax.rem(peer, 2))


def greet(peers):
    barrier = pltpu.get_barrier_semaphore()
    for peer_of in peers:

        def one(i, carry):
            pl.semaphore_signal(barrier, inc=1, device_id=peer_of(i), device_id_type=MESH)
            return carry

        lax.fori_loop(1, NS, one, 0)


def greeted(peers):
    pl.semaphore_wait(pltpu.get_barrier_semaphore(), (NS - 1) * len(peers))


def send(src, dst, send_sem, recv_sem, to):
    pltpu.make_async_remote_copy(
        src_ref=src, dst_ref=dst, send_sem=send_sem, recv_sem=recv_sem, device_id=to, device_id_type=MESH
    ).start()


def await_bytes(ref, sem):
    pltpu.make_async_copy(ref, ref, sem).wait()


def silu(v):
    return v / (1.0 + jnp.exp(-v))


def modulated(tokens, shift, scale):
    values = tokens.astype(F32)
    center = jnp.mean(values, axis=-1, keepdims=True)
    values = values - center
    spread = jnp.mean(values * values, axis=-1, keepdims=True)
    return (values * lax.rsqrt(spread + EPS) * (1.0 + scale) + shift).astype(BF16)


def turned(raw, cos, sin):
    lane = lax.broadcasted_iota(jnp.int32, raw.shape, 1)
    partner = jnp.where(lax.rem(lane, 64) < 32, pltpu.roll(raw, HD - 32, 1), pltpu.roll(raw, 32, 1))
    return (raw * cos + partner * sin).astype(BF16)


def tables():
    inverse = 10000.0 ** (-np.arange(32, dtype=np.float32) / np.float32(32))
    inverse = inverse.astype(np.float32)
    row = (np.arange(128, dtype=np.float32)[:, None] * inverse).astype(np.float32).astype(np.float64)
    col = row[:GRID_W]
    zr, zc = np.zeros((128, 64)), np.zeros((GRID_W, 64))

    def lanes(first, second):
        return np.tile(np.concatenate([first, second], axis=1), (1, 2)).astype(np.float32)

    both = lambda a, b: np.concatenate([a, b], axis=1)
    return (
        lanes(both(np.cos(row), np.cos(row)), zr),
        lanes(both(-np.sin(row), np.sin(row)), zr),
        lanes(zc, both(np.cos(col), np.cos(col))),
        lanes(zc, both(-np.sin(col), np.sin(col))),
    )


def front(
    latent, context, cond, ctx_cond, modulation, wq, wk, wv, rcos, rsin, ccos, csin,
    q_out, kv, ctx, mods, ahead,
    lat, wq_v, wk_v, wv_v, mod_v, ctx_v, parts, normed,
    load, mod_send, mod_recv, ring_send, ring_recv, pair_send, pair_recv,
):
    y, x, z, c = position()
    sp, tp = y * 4 + x, z * 2 + c
    loads = [
        pltpu.make_async_copy(latent, lat.at[z, c], load.at[0]),
        pltpu.make_async_copy(modulation, mod_v, load.at[1]),
        pltpu.make_async_copy(context, ctx_v, load.at[2]),
        pltpu.make_async_copy(wq, wq_v, load.at[3]),
        pltpu.make_async_copy(wk, wk_v, load.at[4]),
        pltpu.make_async_copy(wv, wv_v, load.at[5]),
    ]
    for copy in loads:
        copy.start()

    def half_of(step, way):
        return (0, 1) if step < 4 else ((0,) if way > 0 else (1,))

    def block(rel):
        return lax.rem(z + rel, NZ)

    def ring_step(step, way, half):
        held = block((-way * (step - 1)) % NZ)
        there = (-way * step) % NZ
        rows = pl.ds(half * 16, 16)
        send(
            lat.at[held, c, rows], lat.at[held, c, rows], ring_send.at[there * 2 + half],
            ring_recv.at[there * 2 + half], (y, x, lax.rem(z + way + NZ, NZ), c),
        )

    def ring_wait(rel, half):
        await_bytes(lat.at[block(rel), c, pl.ds(half * 16, 16)], ring_recv.at[rel * 2 + half])

    def pair_step(rel):
        mine = lat.at[block(rel), c]
        send(mine, mine, pair_send.at[rel], pair_recv.at[rel], (y, x, z, 1 - c))

    def pair_wait(rel):
        await_bytes(lat.at[block(rel), 1 - c], pair_recv.at[rel])

    loads[0].wait()
    greeted((sp_peer, tp_peer))
    for half in (0, 1):
        for way in (1, -1):
            ring_step(1, way, half)
    pair_step(0)

    pick = lax.broadcasted_iota(jnp.int32, (8, PART), 0) == 0
    rows = []
    for j in range(2):
        at = pl.ds(sp * 2 + j, 1)
        rows.append(silu(jnp.where(pick, cond[at, :], ctx_cond[at, :])).astype(BF16))
    loads[1].wait()
    for r in range(3):
        product = jnp.dot(rows[0], mod_v[r, 0:PART], preferred_element_type=F32) + jnp.dot(
            rows[1], mod_v[r, PART : 2 * PART], preferred_element_type=F32
        )
        parts[sp, r : r + 1, :] = product[0:1]
        parts[sp, 3 + r : 4 + r, :] = product[1:2]
    parts[sp, 6:8, :] = jnp.zeros((2, HD), F32)

    def show_part(i, carry):
        send(parts.at[sp], parts.at[sp], mod_send.at[0], mod_recv.at[0], sp_peer(i))
        return carry

    lax.fori_loop(1, NS, show_part, 0)
    await_bytes(parts.at[pl.ds(0, NS - 1)], mod_recv.at[0])
    total = parts[0]
    for i in range(1, NS):
        total = total + parts[i]
    own_cols = pl.ds(pl.multiple_of(tp * HD, HD), HD)
    mods[:, own_cols] = total

    def show_sum(i, carry):
        send(mods.at[:, own_cols], mods.at[:, own_cols], mod_send.at[1], mod_recv.at[1], tp_peer(i))
        return carry

    lax.fori_loop(1, NS, show_sum, 0)

    def forward(step):
        for half in (0, 1):
            for way in (1, -1):
                ring_wait((-way * step) % NZ, half)
                if half in half_of(step + 1, way):
                    ring_step(step + 1, way, half)
        for way in (1, -1):
            pair_step((-way * step) % NZ)

    def norm_rows(load_rows, where, pick_mod):
        shift, scale = mods[pick_mod : pick_mod + 1, :], mods[pick_mod + 1 : pick_mod + 2, :]
        for half in (0, 1):
            normed[where + half * 16 : where + half * 16 + 16, :] = modulated(
                load_rows(pl.ds(half * 16, 16)), shift, scale
            )

    def project(units, with_context):
        count = len(units)
        for i, rel in enumerate(units):
            zz = block(rel)
            for core in (0, 1):
                norm_rows(lambda rows, zz=zz, core=core: lat[zz, core, rows, :], i * UNIT + core * ROWS, 0)
        if with_context:
            norm_rows(lambda rows: ctx_v[rows, :], count * UNIT, 3)
        end = count * UNIT + (ROWS if with_context else 0)
        lhs = normed[0:end, :]
        q_raw = jnp.dot(lhs, wq_v[...], preferred_element_type=F32).astype(BF16)
        k_raw = jnp.dot(lhs, wk_v[...], preferred_element_type=F32).astype(BF16)
        v_raw = jnp.dot(lhs, wv_v[...], preferred_element_type=F32).astype(BF16)
        for i, rel in enumerate(units):
            o = PLACE[rel]
            line = pl.ds(sp * NZ + block(rel), 1)
            cos = rcos[line, :] + ccos[...]
            sin = rsin[line, :] + csin[...]
            part = slice(i * UNIT, (i + 1) * UNIT)
            q = turned(q_raw[part].astype(F32), cos, sin)
            for core in (0, 1):
                q_out[core * HD + o * ROWS : core * HD + (o + 1) * ROWS, :] = q[core * ROWS : (core + 1) * ROWS]
            here = pl.ds(pl.multiple_of(sp * UNIT, UNIT), UNIT)
            kv[o, here, 0:HD] = turned(k_raw[part].astype(F32), cos, sin)
            kv[o, here, HD : 2 * HD] = v_raw[part]
        if with_context:
            for o in range(2):
                here = pl.ds(pl.multiple_of(sp * 16, 16), 16)
                part = slice(count * UNIT + o * 16, count * UNIT + o * 16 + 16)
                ctx[o, here, 0:HD] = k_raw[part]
                ctx[o, here, HD : 2 * HD] = v_raw[part]

    forward(1)
    await_bytes(mods.at[:, pl.ds(0, (NS - 1) * HD)], mod_recv.at[1])
    for copy in loads[2:]:
        copy.wait()
    pair_wait(0)
    project([0], True)
    ahead(0)
    forward(2)
    for rel in (7, 1):
        pair_wait(rel)
    project([7, 1], False)
    ahead(1)
    forward(3)
    for rel in (6, 2):
        pair_wait(rel)
    project([6, 2], False)
    ahead(2)
    ring_wait(4, 0)
    ring_wait(4, 1)
    pair_step(4)
    for rel in (5, 3):
        pair_wait(rel)
    project([5, 3], False)
    ahead(3)
    pair_wait(4)
    project([4], False)
    ahead(4)

    await_bytes(parts.at[pl.ds(0, NS - 1)], mod_send.at[0])
    await_bytes(mods.at[:, pl.ds(0, (NS - 1) * HD)], mod_send.at[1])
    for i in range(2, 2 * NZ):
        await_bytes(lat.at[0, 0, pl.ds(0, 16)], ring_send.at[i])
    for rel in range(NZ):
        await_bytes(lat.at[0, 0], pair_send.at[rel])


def gather_unit(kv, tall, kv_send, kv_recv):
    y, x, z, c = position()

    def geometry(o):
        swap = lax.rem(o, 2)
        way = 1 - 2 * lax.rem(o // 2, 2)
        first = swap * y + (1 - swap) * x
        second = swap * x + (1 - swap) * y
        return swap, way, first, second

    def step(o, geo, df, dg, tf, tg, kind):
        swap, way, first, second = geo

        def pair(f, g):
            f, g = lax.rem(f + 8, 4), lax.rem(g + 8, 4)
            return swap * f + (1 - swap) * g, swap * g + (1 - swap) * f

        oy, ox = pair(first + df, second + dg)
        ty, tx = pair(first + tf, second + tg)
        rows = pl.ds(pl.multiple_of((oy * 4 + ox) * tall, tall), tall)
        send(kv.at[o, rows], kv.at[o, rows], kv_send.at[0], kv_recv.at[o * 5 + kind], (ty, tx, z, c))

    def wait(o, kind, count):
        await_bytes(kv.at[o, pl.ds(0, count * tall)], kv_recv.at[o * 5 + kind])

    def own(o):
        geo = geometry(o)
        way = geo[1]
        step(o, geo, 0, 0, 1, 0, 0)
        step(o, geo, 0, 0, -1, 0, 0)
        step(o, geo, 0, 0, 0, way, 1)
        step(o, geo, 0, 0, 0, -way, 4)

    def stage1(o):
        geo = geometry(o)
        way = geo[1]
        wait(o, 0, 2)
        step(o, geo, -way, 0, way, 0, 1)
        for d in (1, -1):
            step(o, geo, d, 0, 0, way, 2)
            step(o, geo, d, 0, 0, -way, 4)

    def stage2(o):
        geo = geometry(o)
        way = geo[1]
        wait(o, 1, 2)
        step(o, geo, 2, 0, 0, way, 3)
        step(o, geo, 2, 0, 0, -way, 4)
        step(o, geo, 0, -way, 0, way, 4)

    def stage3(o):
        geo = geometry(o)
        way = geo[1]
        wait(o, 2, 2)
        for d in (1, -1):
            step(o, geo, d, -way, 0, way, 4)

    def stage4(o):
        geo = geometry(o)
        way = geo[1]
        wait(o, 3, 1)
        step(o, geo, 2, -way, 0, way, 4)

    def done(o):
        wait(o, 4, 8)

    def all_sent():
        await_bytes(kv.at[:, pl.ds(0, (NS - 1) * tall)], kv_send.at[0])

    return own, (stage1, stage2, stage3, stage4), done, all_sent


def absorb(q, m, keys, values, lift, peak, sums, acc):
    scores = lax.dot_general(
        q[:, m * PART : (m + 1) * PART], keys, (((1,), (1,)), ((), ())), preferred_element_type=F32
    )
    scores = scores * (PART**-0.5 * LOG2E)
    if lift is not None:
        scores = scores + lift
    before = peak[m]
    now = jnp.maximum(before, jnp.max(scores, axis=1, keepdims=True))
    fading = jnp.exp2(before - now)
    weights = jnp.exp2(scores - now[:, 0:1])
    sums[m] = sums[m] * fading + jnp.sum(weights, axis=1, keepdims=True)
    acc[m] = acc[m] * fading[:, 0:1] + jnp.dot(weights.astype(BF16), values, preferred_element_type=F32)
    peak[m] = now


CHUNKS = 4
WIDE = D // CHUNKS


def back(
    attended, lat, mods,
    result,
    theirs, wo_v, wo_pair, part, out_buf, in_buf,
    pair_send, pair_recv, out_send, out_recv,
):
    y, x, z, c = position()
    pair = (y, x, z, 1 - c)
    send(attended.at[1 - c], theirs, pair_send.at[0], pair_recv.at[0], pair)
    mine = attended[c]
    await_bytes(theirs, pair_recv.at[0])
    await_bytes(wo_pair, pair_recv.at[1])

    def long_way(j):
        return 0 if j < 2 else 1

    def slot(way, step, j):
        return (way * 4 + step - 1) * CHUNKS + j

    def hop(way, step, j, add):
        rel = (5 - step) if way == 0 else (3 + step) % NZ
        value = part[j, PLACE[rel]]
        if add:
            value = value + in_buf[slot(way, step - 1, j)].astype(F32)
        s = slot(way, step, j)
        out_buf[s] = value.astype(BF16)
        to = lax.rem(z + (1 if way == 0 else NZ - 1), NZ)
        send(out_buf.at[s], in_buf.at[s], out_send.at[s], out_recv.at[s], (y, x, to, c))

    def hop_wait(way, step, j):
        s = slot(way, step, j)
        await_bytes(in_buf.at[s], out_recv.at[s])

    for j in (0, 2, 1, 3):
        cols = slice(j * WIDE, (j + 1) * WIDE)
        product = jnp.dot(mine, wo_v[:, cols], preferred_element_type=F32) + jnp.dot(
            theirs[...], wo_pair[:, cols], preferred_element_type=F32
        )
        part[j] = product.reshape(NZ, ROWS, WIDE)
        hop(long_way(j), 1, j, False)
    for j in (0, 2, 1, 3):
        hop(1 - long_way(j), 2, j, False)
    for step in (1, 2, 3):
        if step > 1:
            for j in (0, 2, 1, 3):
                way = 1 - long_way(j)
                hop_wait(way, step, j)
                hop(way, step + 1, j, True)
        for j in (0, 2, 1, 3):
            way = long_way(j)
            hop_wait(way, step, j)
            hop(way, step + 1, j, True)
    for j in (0, 2, 1, 3):
        cols = slice(j * WIDE, (j + 1) * WIDE)
        total = part[j, 0]
        for way in (1 - long_way(j), long_way(j)):
            hop_wait(way, 4, j)
            total = total + in_buf[slot(way, 4, j)].astype(F32)
        result[:, cols] = (lat[z, c, :, cols].astype(F32) + mods[2:3, cols] * total).astype(BF16)
    await_bytes(theirs, pair_send.at[0])
    await_bytes(wo_pair, pair_send.at[1])
    for way in (0, 1):
        for step in (1, 2, 3, 4):
            for j in range(CHUNKS):
                if step > 1 or long_way(j) == way:
                    s = slot(way, step, j)
                    await_bytes(out_buf.at[s], out_send.at[s])


def kernel(
    latent, context, cond, ctx_cond, modulation, wq, wk, wv, rcos, rsin, ccos, csin, lift, lam, gain, wo,
    result,
    lat, wq_v, wk_v, wv_v, mod_v, ctx_v, parts, normed, mods,
    q, kv, ctx, peak, sums, acc, attended,
    theirs, wo_v, wo_pair, part, out_buf, in_buf,
    load, mod_send, mod_recv, ring_send, ring_recv, pair_send, pair_recv,
    kv_send, kv_recv, ctx_send, ctx_recv,
    back_load, back_send, back_recv, out_send, out_recv,
):
    y, x, z, c = position()
    greet((sp_peer, tp_peer))
    wo_copy = pltpu.make_async_copy(wo, wo_v, back_load.at[0])
    own, stages, done, all_sent = gather_unit(kv, UNIT, kv_send, kv_recv)
    ctx_own, ctx_stages, ctx_done, ctx_all_sent = gather_unit(ctx, 16, ctx_send, ctx_recv)
    peak[...] = jnp.full(peak.shape, -jnp.inf, F32)
    sums[...] = jnp.zeros(sums.shape, F32)
    acc[...] = jnp.zeros(acc.shape, F32)

    def over(count, one, first=0):
        lax.fori_loop(first, first + count, lambda o, carry: (one(o), carry)[1], 0)

    def ahead(step):
        if step == 0:
            own(0)
            over(2, ctx_own)
            wo_copy.start()
        if step == 1:
            over(2, own, 1)
            over(2, ctx_stages[0])
            stages[0](0)
            wo_copy.wait()
            send(wo_v, wo_pair, back_send.at[1], back_recv.at[1], (y, x, z, 1 - c))
        if step == 2:
            over(2, own, 3)
            over(2, ctx_stages[1])
            stages[0](1)
            stages[1](0)
        if step == 3:
            over(2, own, 5)
            over(2, ctx_stages[2])
            over(2, ctx_stages[3])
            stages[0](2)
            stages[1](1)
            stages[2](0)
        if step == 4:
            own(7)

    front(
        latent, context, cond, ctx_cond, modulation, wq, wk, wv, rcos, rsin, ccos, csin,
        q, kv, ctx, mods, ahead,
        lat, wq_v, wk_v, wv_v, mod_v, ctx_v, parts, normed,
        load, mod_send, mod_recv, ring_send, ring_recv, pair_send, pair_recv,
    )
    lift_term = lift[0] * LOG2E
    lag = 5

    def tick(t, carry):
        def stage(k):
            o = t - k

            @pl.when((o >= 0) & (o < NZ))
            def _():
                stages[k](o)

        def attend(m):
            o = t - lag

            @pl.when(o >= 0)
            def _():
                if m == 0:
                    done(o)
                absorb(q, m, kv[o, :, m * PART : (m + 1) * PART], kv[o, :, HD : 2 * HD], None, peak, sums, acc)

        stage(0)
        attend(0)
        stage(1)
        stage(2)
        attend(1)
        stage(3)

        @pl.when(t == 3)
        def _():
            over(2, ctx_done)
            for m in range(2):
                absorb(
                    q, m, ctx[:, :, m * PART : (m + 1) * PART].reshape(NS * ROWS, PART),
                    ctx[:, :, HD : 2 * HD].reshape(NS * ROWS, HD), lift_term, peak, sums, acc,
                )

        return carry

    lax.fori_loop(3, NZ + lag, tick, 0)
    means = [acc[m] / sums[m][:, 0:1] for m in range(2)]
    difference = means[0] - lam[0] * means[1]
    spread = jnp.mean(difference * difference, axis=1, keepdims=True)
    final = (difference * lax.rsqrt(spread + EPS) * gain[...]).astype(BF16)
    attended[0] = final[0:HD]
    attended[1] = final[HD : 2 * HD]
    back(
        attended, lat, mods, result, theirs, wo_v, wo_pair, part, out_buf, in_buf,
        back_send, back_recv, out_send, out_recv,
    )
    all_sent()
    ctx_all_sent()


def run(*arrays):
    dma = pltpu.SemaphoreType.DMA
    slots = 2 * 4 * CHUNKS
    return pl.pallas_call(
        kernel,
        out_shape=jax.ShapeDtypeStruct((ROWS, D), BF16),
        in_specs=[ANY, ANY, VM, VM, ANY, ANY, ANY, ANY, VM, VM, VM, VM, SM, SM, VM, ANY],
        out_specs=VM,
        scratch_shapes=[
            pltpu.VMEM((NZ, 2, ROWS, D), BF16),
            pltpu.VMEM((D, HD), BF16),
            pltpu.VMEM((D, HD), BF16),
            pltpu.VMEM((D, HD), BF16),
            pltpu.VMEM((3, HD, HD), BF16),
            pltpu.VMEM((ROWS, D), BF16),
            pltpu.VMEM((NS, 8, HD), F32),
            pltpu.VMEM((2 * UNIT, D), BF16),
            pltpu.VMEM((8, D), F32),
            pltpu.VMEM((BLOCK, HD), BF16),
            pltpu.VMEM((NZ, NS * UNIT, 2 * HD), BF16),
            pltpu.VMEM((2, NS * 16, 2 * HD), BF16),
            pltpu.VMEM((2, BLOCK, 128), F32),
            pltpu.VMEM((2, BLOCK, 128), F32),
            pltpu.VMEM((2, BLOCK, HD), F32),
            pltpu.VMEM((2, HD, HD), BF16),
            pltpu.VMEM((HD, HD), BF16),
            pltpu.VMEM((HD, D), BF16),
            pltpu.VMEM((HD, D), BF16),
            pltpu.VMEM((CHUNKS, NZ, ROWS, WIDE), F32),
            pltpu.VMEM((slots, ROWS, WIDE), BF16),
            pltpu.VMEM((slots, ROWS, WIDE), BF16),
            dma((6,)),
            dma((2,)),
            dma((2,)),
            dma((2 * NZ,)),
            dma((2 * NZ,)),
            dma((NZ,)),
            dma((NZ,)),
            dma((1,)),
            dma((5 * NZ,)),
            dma((1,)),
            dma((10,)),
            dma((1,)),
            dma((2,)),
            dma((2,)),
            dma((slots,)),
            dma((slots,)),
        ],
        compiler_params=pltpu.CompilerParams(
            collective_id=0, has_side_effects=True, vmem_limit_bytes=60 * 2**20
        ),
        name="whole",
    )(*arrays)


def shards(
    latent, context, condition, context_condition, modulation,
    query_weight, key_weight, value_weight, lambdas, context_lift, head_gain, output_weight,
):
    return run(
        latent, context, condition.reshape(32, 128), context_condition.reshape(32, 128),
        modulation, query_weight, key_weight, value_weight, *[jnp.asarray(t) for t in tables()],
        context_lift, lambdas, head_gain.reshape(1, HD), output_weight,
    )


def solution(mesh):
    split = Mesh(mesh.devices.reshape(4, 4, NZ, 2), ("y", "x", "z", "c"))
    sp, tp = ("y", "x"), ("z", "c")
    return jax.shard_map(
        shards,
        mesh=split,
        in_specs=(
            P(sp + tp, None),
            P(sp, None),
            P(),
            P(),
            P(None, sp, tp),
            P(None, tp),
            P(None, tp),
            P(None, tp),
            P(tp),
            P(tp),
            P(),
            P(tp, None),
        ),
        out_specs=P(sp + tp, None),
        check_vma=False,
    )
```

```python
import functools
import math

import jax
import jax.numpy as jnp
import numpy as np
from jax import lax
from jax.experimental import pallas as pl
from jax.experimental.pallas import tpu as pltpu
from jax.sharding import Mesh
from jax.sharding import PartitionSpec as P

MESH = pl.DeviceIdType.MESH
F32 = jnp.float32
BF16 = jnp.bfloat16
GRID_W = 64
EPS = 1e-5
NZ = 8
NS = 16
D = 4096
HD = 256
PART = 128
ROWS = 32
LOG2E = math.log2(math.e)
ORDER = (0, 7, 1, 6, 2, 5, 3, 4)
PLACE = {rel: i for i, rel in enumerate(ORDER)}
UNIT = 2 * ROWS
SLOTS_AHEAD = (0, 0, 2, 3, 4, 5)
BLOCK = NZ * UNIT
ANY = pl.BlockSpec(memory_space=pl.ANY)
VM = pl.BlockSpec(memory_space=pltpu.VMEM)
SM = pl.BlockSpec(memory_space=pltpu.SMEM)


def position():
    return tuple(lax.axis_index(a) for a in ("y", "x", "z", "c"))


def sp_peer(i):
    y, x, z, c = position()
    peer = lax.rem(y * 4 + x + i, NS)
    return (peer // 4, lax.rem(peer, 4), z, c)


def tp_peer(i):
    y, x, z, c = position()
    peer = lax.rem(z * 2 + c + i, NS)
    return (y, x, peer // 2, lax.rem(peer, 2))


def greet(peers):
    barrier = pltpu.get_barrier_semaphore()
    for peer_of in peers:

        def one(i, carry):
            pl.semaphore_signal(barrier, inc=1, device_id=peer_of(i), device_id_type=MESH)
            return carry

        lax.fori_loop(1, NS, one, 0)


    y, x, z, c = position()
    pl.semaphore_signal(barrier, inc=1, device_id=(y, 3 - x, z, 1 - c), device_id_type=MESH)


def greeted(peers):
    pl.semaphore_wait(pltpu.get_barrier_semaphore(), (NS - 1) * len(peers) + 1)


def send(src, dst, send_sem, recv_sem, to):
    pltpu.make_async_remote_copy(
        src_ref=src, dst_ref=dst, send_sem=send_sem, recv_sem=recv_sem, device_id=to, device_id_type=MESH
    ).start()


def await_bytes(ref, sem):
    pltpu.make_async_copy(ref, ref, sem).wait()


def silu(v):
    return v / (1.0 + jnp.exp(-v))


def modulated(tokens, shift, scale):
    values = tokens.astype(F32)
    center = jnp.mean(values, axis=-1, keepdims=True)
    values = values - center
    spread = jnp.mean(values * values, axis=-1, keepdims=True)
    return (values * lax.rsqrt(spread + EPS) * (1.0 + scale) + shift).astype(BF16)


def turned(raw, cos, sin):
    lane = lax.broadcasted_iota(jnp.int32, raw.shape, 1)
    partner = jnp.where(lax.rem(lane, 64) < 32, pltpu.roll(raw, HD - 32, 1), pltpu.roll(raw, 32, 1))
    return (raw * cos + partner * sin).astype(BF16)


def tables():
    inverse = 10000.0 ** (-np.arange(32, dtype=np.float32) / np.float32(32))
    inverse = inverse.astype(np.float32)
    row = (np.arange(128, dtype=np.float32)[:, None] * inverse).astype(np.float32).astype(np.float64)
    col = row[:GRID_W]
    zr, zc = np.zeros((128, 64)), np.zeros((GRID_W, 64))

    def lanes(first, second):
        return np.tile(np.concatenate([first, second], axis=1), (1, 2)).astype(np.float32)

    both = lambda a, b: np.concatenate([a, b], axis=1)
    return (
        lanes(both(np.cos(row), np.cos(row)), zr),
        lanes(both(-np.sin(row), np.sin(row)), zr),
        lanes(zc, both(np.cos(col), np.cos(col))),
        lanes(zc, both(-np.sin(col), np.sin(col))),
    )


def front(
    latent, context, cond, ctx_cond, modulation, wq, wk, wv, rcos, rsin, ccos, csin,
    q, kv, ctx, kv_away, ctx_away, mods, ahead, early,
    lat, wq_v, wk_v, wv_v, mod_v, ctx_v, parts, normed,
    load, mod_send, mod_recv, ring_send, ring_recv, pair_send, pair_recv,
):
    y, x, z, c = position()
    sp, tp = y * 4 + x, z * 2 + c
    right = c == x // 2
    seat = lax.rem(x, 2) * 4 + y
    loads = [
        pltpu.make_async_copy(latent, lat.at[z, c], load.at[0]),
        pltpu.make_async_copy(modulation, mod_v, load.at[1]),
        pltpu.make_async_copy(context, ctx_v, load.at[2]),
        pltpu.make_async_copy(wq, wq_v, load.at[3]),
        pltpu.make_async_copy(wk, wk_v, load.at[4]),
        pltpu.make_async_copy(wv, wv_v, load.at[5]),
    ]
    for copy in loads:
        copy.start()

    def half_of(step, way):
        return (0, 1) if step < 4 else ((0,) if way > 0 else (1,))

    def block(rel):
        return lax.rem(z + rel, NZ)

    def ring_step(step, way, half):
        held = block((-way * (step - 1)) % NZ)
        there = (-way * step) % NZ
        rows = pl.ds(half * 16, 16)
        send(
            lat.at[held, c, rows], lat.at[held, c, rows], ring_send.at[there * 2 + half],
            ring_recv.at[there * 2 + half], (y, x, lax.rem(z + way + NZ, NZ), c),
        )

    def ring_wait(rel, half):
        await_bytes(lat.at[block(rel), c, pl.ds(half * 16, 16)], ring_recv.at[rel * 2 + half])

    def pair_step(rel):
        mine = lat.at[block(rel), c]
        send(mine, mine, pair_send.at[rel], pair_recv.at[rel], (y, x, z, 1 - c))

    def pair_wait(rel):
        await_bytes(lat.at[block(rel), 1 - c], pair_recv.at[rel])

    loads[0].wait()
    greeted((sp_peer, tp_peer))
    early()
    for half in (0, 1):
        for way in (1, -1):
            ring_step(1, way, half)
    pair_step(0)

    pick = lax.broadcasted_iota(jnp.int32, (8, PART), 0) == 0
    rows = []
    for j in range(2):
        at = pl.ds(sp * 2 + j, 1)
        rows.append(silu(jnp.where(pick, cond[at, :], ctx_cond[at, :])).astype(BF16))
    loads[1].wait()
    for r in range(3):
        product = jnp.dot(rows[0], mod_v[r, 0:PART], preferred_element_type=F32) + jnp.dot(
            rows[1], mod_v[r, PART : 2 * PART], preferred_element_type=F32
        )
        parts[sp, r : r + 1, :] = product[0:1]
        parts[sp, 3 + r : 4 + r, :] = product[1:2]
    parts[sp, 6:8, :] = jnp.zeros((2, HD), F32)

    def show_part(i, carry):
        send(parts.at[sp], parts.at[sp], mod_send.at[0], mod_recv.at[0], sp_peer(i))
        return carry

    lax.fori_loop(1, NS, show_part, 0)
    await_bytes(parts.at[pl.ds(0, NS - 1)], mod_recv.at[0])
    total = parts[0]
    for i in range(1, NS):
        total = total + parts[i]
    own_cols = pl.ds(pl.multiple_of(tp * HD, HD), HD)
    mods[:, own_cols] = total

    def show_sum(i, carry):
        send(mods.at[:, own_cols], mods.at[:, own_cols], mod_send.at[1], mod_recv.at[1], tp_peer(i))
        return carry

    lax.fori_loop(1, NS, show_sum, 0)

    def forward(step):
        for half in (0, 1):
            for way in (1, -1):
                ring_wait((-way * step) % NZ, half)
                if half in half_of(step + 1, way):
                    ring_step(step + 1, way, half)
        for way in (1, -1):
            pair_step((-way * step) % NZ)

    def norm_rows(load_rows, where, pick_mod):
        shift, scale = mods[pick_mod : pick_mod + 1, :], mods[pick_mod + 1 : pick_mod + 2, :]
        for half in (0, 1):
            normed[where + half * 16 : where + half * 16 + 16, :] = modulated(
                load_rows(pl.ds(half * 16, 16)), shift, scale
            )

    def project(units, with_context):
        count = len(units)
        for i, rel in enumerate(units):
            zz = block(rel)
            for core in (0, 1):
                norm_rows(lambda rows, zz=zz, core=core: lat[zz, core, rows, :], i * UNIT + core * ROWS, 0)
        if with_context:
            norm_rows(lambda rows: ctx_v[rows, :], count * UNIT, 3)
        end = count * UNIT + (ROWS if with_context else 0)
        lhs = normed[0:end, :]
        q_raw = jnp.dot(lhs, wq_v[...], preferred_element_type=F32).astype(BF16)
        k_raw = jnp.dot(lhs, wk_v[...], preferred_element_type=F32).astype(BF16)
        v_raw = jnp.dot(lhs, wv_v[...], preferred_element_type=F32).astype(BF16)
        for i, rel in enumerate(units):
            o = PLACE[rel]
            line = pl.ds(sp * NZ + block(rel), 1)
            cos = rcos[line, :] + ccos[...]
            sin = rsin[line, :] + csin[...]
            part = slice(i * UNIT, (i + 1) * UNIT)
            q[0, o * UNIT : (o + 1) * UNIT, :] = turned(q_raw[part].astype(F32), cos, sin)
            keys = turned(k_raw[part].astype(F32), cos, sin)

            @pl.when(right)
            def _():
                here = pl.ds(pl.multiple_of(seat * UNIT, UNIT), UNIT)
                kv[c, o, here, 0:HD] = keys
                kv[c, o, here, HD : 2 * HD] = v_raw[part]

            @pl.when(jnp.logical_not(right))
            def _():
                kv_away[o, :, 0:HD] = keys
                kv_away[o, :, HD : 2 * HD] = v_raw[part]

        if with_context:

            @pl.when(right)
            def _():
                here = pl.ds(pl.multiple_of(seat * ROWS, ROWS), ROWS)
                ctx[c, 0, here, 0:HD] = k_raw[count * UNIT : end]
                ctx[c, 0, here, HD : 2 * HD] = v_raw[count * UNIT : end]

            @pl.when(jnp.logical_not(right))
            def _():
                ctx_away[:, 0:HD] = k_raw[count * UNIT : end]
                ctx_away[:, HD : 2 * HD] = v_raw[count * UNIT : end]

    forward(1)
    forward(2)
    await_bytes(mods.at[:, pl.ds(0, (NS - 1) * HD)], mod_recv.at[1])
    for copy in loads[2:]:
        copy.wait()
    pair_wait(0)
    project([0], True)
    ahead(0)
    for rel in (7, 1):
        pair_wait(rel)
    project([7, 1], False)
    ahead(1)
    forward(3)
    for rel in (6, 2):
        pair_wait(rel)
    project([6, 2], False)
    ahead(2)
    ring_wait(4, 0)
    ring_wait(4, 1)
    pair_step(4)
    for rel in (5, 3):
        pair_wait(rel)
    project([5, 3], False)
    ahead(3)
    pair_wait(4)
    project([4], False)
    ahead(4)

    await_bytes(parts.at[pl.ds(0, NS - 1)], mod_send.at[0])
    await_bytes(mods.at[:, pl.ds(0, (NS - 1) * HD)], mod_send.at[1])
    for i in range(2, 2 * NZ):
        await_bytes(lat.at[0, 0, pl.ds(0, 16)], ring_send.at[i])
    for rel in range(NZ):
        await_bytes(lat.at[0, 0], pair_send.at[rel])


def gather_unit(kv, tall, kv_send, kv_recv):
    y, x, z, c = position()
    mate = x + 1 - 2 * lax.rem(x, 2)

    def wrap(v):
        return lax.rem(v + 8, 4)

    def way_of(o):
        return 1 - 2 * lax.rem(o // 2, 2)

    def step(o, crossed, dy, over, ty, kind):
        ox = mate if crossed else x
        seat = lax.rem(ox, 2) * 4 + wrap(y + dy)
        rows = pl.ds(pl.multiple_of(seat * tall, tall), tall)
        send(
            kv.at[c, o, rows], kv.at[c, o, rows], kv_send.at[0], kv_recv.at[o * 4 + kind],
            (wrap(y + ty), mate if over else x, z, c),
        )

    def wait(o, kind, count=1):
        await_bytes(kv.at[c, o, pl.ds(0, count * tall)], kv_recv.at[o * 4 + kind])

    def typed(o, even, odd):
        if isinstance(o, int):
            (odd if o % 2 else even)()
        else:
            pl.when(lax.rem(o, 2) == 0)(even)
            pl.when(lax.rem(o, 2) == 1)(odd)

    def own(o):
        way = way_of(o)

        def even():
            step(o, False, 0, True, 0, 0)
            step(o, False, 0, False, way, 1)
            step(o, False, 0, False, -way, 3)

        def odd():
            step(o, False, 0, False, way, 1)
            step(o, False, 0, False, -way, 0)
            step(o, False, 0, True, 0, 3)

        typed(o, even, odd)

    def stage1(o):
        way = way_of(o)

        def even():
            wait(o, 0)
            step(o, True, 0, False, way, 2)
            step(o, True, 0, False, -way, 3)

        def odd():
            wait(o, 1)
            step(o, False, -way, False, way, 2)
            step(o, False, -way, True, 0, 3)
            wait(o, 0)
            step(o, False, way, True, 0, 3)

        typed(o, even, odd)

    def stage2(o):
        way = way_of(o)

        def even():
            wait(o, 1)
            step(o, False, -way, False, way, 3)

        def odd():
            wait(o, 2)
            step(o, False, 2, True, 0, 3)

        typed(o, even, odd)

    def stage3(o):
        way = way_of(o)

        def even():
            wait(o, 2)
            step(o, True, -way, False, way, 3)

        typed(o, even, lambda: None)

    def done(o):
        wait(o, 3, 4)

    def all_sent(units):
        for o in range(units):
            await_bytes(kv.at[0, 0, pl.ds(0, 7 * tall)], kv_send.at[0])

    return own, (stage1, stage2, stage3), done, all_sent


def absorb(q, m, keys, values, lift, peak, sums, acc):
    scores = lax.dot_general(
        q, keys, (((1,), (1,)), ((), ())), preferred_element_type=F32
    )
    scores = scores * (PART**-0.5 * LOG2E)
    if lift is not None:
        scores = scores + lift
    before = peak[m]
    now = jnp.maximum(before, jnp.max(scores, axis=1, keepdims=True))
    fading = jnp.exp2(before - now)
    weights = jnp.exp2(scores - now[:, 0:1])
    sums[m] = sums[m] * fading + jnp.sum(weights, axis=1, keepdims=True)
    acc[m] = acc[m] * fading[:, 0:1] + jnp.dot(weights.astype(BF16), values, preferred_element_type=F32)
    peak[m] = now


CHUNKS = 4
WIDE = D // CHUNKS


def back(
    heads, lat, mods,
    result,
    wo_v, wo_pair, part, out_buf, in_buf,
    pair_send, pair_recv, out_send, out_recv,
):
    y, x, z, c = position()
    mine, theirs = heads[0], heads[1]
    await_bytes(wo_pair, pair_recv.at[1])

    def long_way(j):
        return 0 if j < 2 else 1

    def slot(way, step, j):
        return (way * 4 + step - 1) * CHUNKS + j

    def hop(way, step, j, add):
        rel = (5 - step) if way == 0 else (3 + step) % NZ
        value = part[j, PLACE[rel]]
        if add:
            value = value + in_buf[slot(way, step - 1, j)].astype(F32)
        s = slot(way, step, j)
        out_buf[s] = value.astype(BF16)
        to = lax.rem(z + (1 if way == 0 else NZ - 1), NZ)
        send(out_buf.at[s], in_buf.at[s], out_send.at[s], out_recv.at[s], (y, x, to, c))

    def hop_wait(way, step, j):
        s = slot(way, step, j)
        await_bytes(in_buf.at[s], out_recv.at[s])

    for j in (0, 2, 1, 3):
        cols = slice(j * WIDE, (j + 1) * WIDE)
        product = jnp.dot(mine, wo_v[:, cols], preferred_element_type=F32) + jnp.dot(
            theirs, wo_pair[:, cols], preferred_element_type=F32
        )
        part[j] = product.reshape(NZ, ROWS, WIDE)
        hop(long_way(j), 1, j, False)
    for j in (0, 2, 1, 3):
        hop(1 - long_way(j), 2, j, False)
    for step in (1, 2, 3):
        if step > 1:
            for j in (0, 2, 1, 3):
                way = 1 - long_way(j)
                hop_wait(way, step, j)
                hop(way, step + 1, j, True)
        for j in (0, 2, 1, 3):
            way = long_way(j)
            hop_wait(way, step, j)
            hop(way, step + 1, j, True)
    for j in (0, 2, 1, 3):
        cols = slice(j * WIDE, (j + 1) * WIDE)
        total = part[j, 0]
        for way in (1 - long_way(j), long_way(j)):
            hop_wait(way, 4, j)
            total = total + in_buf[slot(way, 4, j)].astype(F32)
        result[:, cols] = (lat[z, c, :, cols].astype(F32) + mods[2:3, cols] * total).astype(BF16)
    await_bytes(wo_pair, pair_send.at[1])
    for way in (0, 1):
        for step in (1, 2, 3, 4):
            for j in range(CHUNKS):
                if step > 1 or long_way(j) == way:
                    s = slot(way, step, j)
                    await_bytes(out_buf.at[s], out_send.at[s])


def kernel(
    latent, context, cond, ctx_cond, modulation, wq, wk, wv, rcos, rsin, ccos, csin, lift, lam, gain, wo,
    result,
    lat, wq_v, wk_v, wv_v, mod_v, ctx_v, parts, normed, mods,
    q, kv, ctx, kv_away, ctx_away, settings, peak, sums, acc, attended, heads,
    wo_v, wo_pair, part, out_buf, in_buf,
    load, mod_send, mod_recv, ring_send, ring_recv, pair_send, pair_recv,
    kv_send, kv_recv, ctx_send, ctx_recv, away_send, away_recv, lane_send, lane_recv, set_send, set_recv,
    head_send, head_recv, back_load, back_send, back_recv, out_send, out_recv,
):
    y, x, z, c = position()
    greet((sp_peer, tp_peer))
    group = x // 2
    right = c == group
    wrong = c != group
    partner = (y, 3 - x, z, 1 - c)
    sibling = (y, x, z, 1 - c)
    wo_copy = pltpu.make_async_copy(wo, wo_v, back_load.at[0])
    own, stages, done, all_sent = gather_unit(kv, UNIT, kv_send, kv_recv)
    ctx_own, ctx_stages, ctx_done, ctx_all_sent = gather_unit(ctx, ROWS, ctx_send, ctx_recv)
    settings[0, 0] = jnp.full((8, 128), lift[0] * LOG2E, F32)
    settings[0, 1] = jnp.full((8, 128), lam[0], F32)
    peak[...] = jnp.full(peak.shape, -jnp.inf, F32)
    sums[...] = jnp.zeros(sums.shape, F32)
    acc[...] = jnp.zeros(acc.shape, F32)
    there = lax.rem(3 - x, 2) * 4 + y
    here = lax.rem(x, 2) * 4 + y

    def early():
        send(settings.at[0], settings.at[1], set_send.at[0], set_recv.at[0], sibling)

    def away(*units):
        @pl.when(wrong)
        def _():
            for o in units:
                rows = pl.ds(o * UNIT, UNIT)
                send(q.at[0, rows], q.at[1, rows], away_send.at[0], away_recv.at[NZ + 1], partner)
                send(
                    kv_away.at[o], kv.at[1 - c, o, pl.ds(pl.multiple_of(there * UNIT, UNIT), UNIT)],
                    away_send.at[1], away_recv.at[o], partner,
                )

    def ctx_away_start():
        @pl.when(wrong)
        def _():
            send(
                ctx_away, ctx.at[1 - c, 0, pl.ds(pl.multiple_of(there * ROWS, ROWS), ROWS)],
                away_send.at[2], away_recv.at[NZ], partner,
            )

    def begin(o):
        @pl.when(wrong)
        def _():
            await_bytes(kv.at[0, 0, pl.ds(0, UNIT)], away_recv.at[o])

        own(o)

    def ctx_begin(o):
        @pl.when(wrong)
        def _():
            await_bytes(ctx.at[0, 0, pl.ds(0, ROWS)], away_recv.at[NZ])

        ctx_own(o)

    def show_lane(o):
        done(o)
        send(kv.at[c, o], kv.at[c, o], lane_send.at[0], lane_recv.at[o], sibling)

    def ctx_show_lane(o):
        ctx_done(o)
        send(ctx.at[c], ctx.at[c], lane_send.at[1], lane_recv.at[NZ], sibling)

    choice = jnp.where(right, 0, 1)

    def attend(m):
        def one(o):
            if m == 0:
                await_bytes(kv.at[0, 0], lane_recv.at[o])
            absorb(
                q[choice, :, m * PART : (m + 1) * PART], m,
                kv[:, o, :, m * PART : (m + 1) * PART].reshape(NS * UNIT, PART),
                kv[:, o, :, HD : 2 * HD].reshape(NS * UNIT, HD), None, peak, sums, acc,
            )

        return one

    def ctx_attend(o):
        await_bytes(ctx.at[0], lane_recv.at[NZ])
        lift_term = settings[choice, 0, 0:1, 0:1]
        for m in range(2):
            absorb(
                q[choice, :, m * PART : (m + 1) * PART], m,
                ctx[:, 0, :, m * PART : (m + 1) * PART].reshape(NS * ROWS, PART),
                ctx[:, 0, :, HD : 2 * HD].reshape(NS * ROWS, HD), lift_term, peak, sums, acc,
            )

    steps = (
        (3, stages[2]), (0, begin), (5, attend(0)), (4, show_lane), (1, stages[0]), (2, stages[1]), (5, attend(1)),
    )
    ctx_steps = {
        1: ctx_begin, 2: ctx_stages[0], 3: ctx_stages[1], 4: ctx_stages[2], 5: ctx_show_lane, 6: ctx_attend,
    }

    def slot(t):
        for after, one in steps:
            o = t - after
            if isinstance(t, int):
                if 0 <= o < NZ:
                    one(o)
            else:

                @pl.when((o >= 0) & (o < NZ))
                def _(o=o, one=one):
                    one(o)

        for at, one in ctx_steps.items():
            if isinstance(t, int):
                if t == at:
                    one(0)
            elif at >= SLOTS_AHEAD[-1]:

                @pl.when(t == at)
                def _(one=one):
                    one(0)

    def ahead(step):
        if step == 0:
            away(0)
            ctx_away_start()
            wo_copy.start()
        else:
            away(*((2 * step - 1, 2 * step) if step < 4 else (7,)))
        for t in range(SLOTS_AHEAD[step], SLOTS_AHEAD[step + 1]):
            slot(t)
        if step == 1:
            wo_copy.wait()
            send(wo_v, wo_pair, back_send.at[1], back_recv.at[1], sibling)

    front(
        latent, context, cond, ctx_cond, modulation, wq, wk, wv, rcos, rsin, ccos, csin,
        q, kv, ctx, kv_away, ctx_away, mods, ahead, early,
        lat, wq_v, wk_v, wv_v, mod_v, ctx_v, parts, normed,
        load, mod_send, mod_recv, ring_send, ring_recv, pair_send, pair_recv,
    )
    await_bytes(settings.at[1], set_recv.at[0])

    @pl.when(wrong)
    def _():
        await_bytes(q.at[1], away_recv.at[NZ + 1])

    def later(t, carry):
        slot(t)
        return carry

    lax.fori_loop(SLOTS_AHEAD[-1], NZ + 5, later, 0)
    lam_term = settings[choice, 1, 0:1, 0:1]
    means = [acc[m] / sums[m][:, 0:1] for m in range(2)]
    difference = means[0] - lam_term * means[1]
    spread = jnp.mean(difference * difference, axis=1, keepdims=True)
    final = (difference * lax.rsqrt(spread + EPS) * gain[...]).astype(BF16).reshape(NZ, 2, ROWS, HD)
    for core in (0, 1):
        attended[core] = final[:, core].reshape(HD, HD)

    @pl.when(right)
    def _():
        heads[0] = attended[c]
        send(attended.at[1 - c], heads.at[1], head_send.at[0], head_recv.at[0], sibling)
        await_bytes(heads.at[0], head_recv.at[1])

    @pl.when(wrong)
    def _():
        for core in (0, 1):
            slot = jnp.where(c == core, 1, 0)
            send(
                attended.at[core], heads.at[slot], head_send.at[core], head_recv.at[1], (y, 3 - x, z, core)
            )
        await_bytes(heads.at[0], head_recv.at[0])
        await_bytes(heads.at[0], head_recv.at[1])

    back(
        heads, lat, mods, result, wo_v, wo_pair, part, out_buf, in_buf,
        back_send, back_recv, out_send, out_recv,
    )
    all_sent(NZ)
    ctx_all_sent(1)
    await_bytes(settings.at[0], set_send.at[0])
    await_bytes(ctx.at[0], lane_send.at[1])
    for o in range(NZ):
        await_bytes(kv.at[0, 0], lane_send.at[0])
    await_bytes(heads.at[0], head_send.at[0])

    @pl.when(wrong)
    def _():
        await_bytes(heads.at[0], head_send.at[1])
        await_bytes(q.at[0], away_send.at[0])
        await_bytes(kv_away, away_send.at[1])
        await_bytes(ctx_away, away_send.at[2])


def run(*arrays):
    dma = pltpu.SemaphoreType.DMA
    slots = 2 * 4 * CHUNKS
    return pl.pallas_call(
        kernel,
        out_shape=jax.ShapeDtypeStruct((ROWS, D), BF16),
        in_specs=[ANY, ANY, VM, VM, ANY, ANY, ANY, ANY, VM, VM, VM, VM, SM, SM, VM, ANY],
        out_specs=VM,
        scratch_shapes=[
            pltpu.VMEM((NZ, 2, ROWS, D), BF16),
            pltpu.VMEM((D, HD), BF16),
            pltpu.VMEM((D, HD), BF16),
            pltpu.VMEM((D, HD), BF16),
            pltpu.VMEM((3, HD, HD), BF16),
            pltpu.VMEM((ROWS, D), BF16),
            pltpu.VMEM((NS, 8, HD), F32),
            pltpu.VMEM((2 * UNIT, D), BF16),
            pltpu.VMEM((8, D), F32),
            pltpu.VMEM((2, BLOCK, HD), BF16),
            pltpu.VMEM((2, NZ, NS // 2 * UNIT, 2 * HD), BF16),
            pltpu.VMEM((2, 1, NS // 2 * ROWS, 2 * HD), BF16),
            pltpu.VMEM((NZ, UNIT, 2 * HD), BF16),
            pltpu.VMEM((ROWS, 2 * HD), BF16),
            pltpu.VMEM((2, 2, 8, 128), F32),
            pltpu.VMEM((2, BLOCK, 128), F32),
            pltpu.VMEM((2, BLOCK, 128), F32),
            pltpu.VMEM((2, BLOCK, HD), F32),
            pltpu.VMEM((2, HD, HD), BF16),
            pltpu.VMEM((2, HD, HD), BF16),
            pltpu.VMEM((HD, D), BF16),
            pltpu.VMEM((HD, D), BF16),
            pltpu.VMEM((CHUNKS, NZ, ROWS, WIDE), F32),
            pltpu.VMEM((slots, ROWS, WIDE), BF16),
            pltpu.VMEM((slots, ROWS, WIDE), BF16),
            dma((6,)),
            dma((2,)),
            dma((2,)),
            dma((2 * NZ,)),
            dma((2 * NZ,)),
            dma((NZ,)),
            dma((NZ,)),
            dma((1,)),
            dma((4 * NZ,)),
            dma((1,)),
            dma((4,)),
            dma((3,)),
            dma((NZ + 2,)),
            dma((2,)),
            dma((NZ + 1,)),
            dma((1,)),
            dma((1,)),
            dma((2,)),
            dma((2,)),
            dma((1,)),
            dma((2,)),
            dma((2,)),
            dma((slots,)),
            dma((slots,)),
        ],
        compiler_params=pltpu.CompilerParams(
            collective_id=0, has_side_effects=True, vmem_limit_bytes=60 * 2**20
        ),
        name="whole",
    )(*arrays)


def shards(
    latent, context, condition, context_condition, modulation,
    query_weight, key_weight, value_weight, lambdas, context_lift, head_gain, output_weight,
):
    return run(
        latent, context, condition.reshape(32, 128), context_condition.reshape(32, 128),
        modulation, query_weight, key_weight, value_weight, *[jnp.asarray(t) for t in tables()],
        context_lift, lambdas, head_gain.reshape(1, HD), output_weight,
    )


def solution(mesh):
    split = Mesh(mesh.devices.reshape(4, 4, NZ, 2), ("y", "x", "z", "c"))
    sp, tp = ("y", "x"), ("z", "c")
    return jax.shard_map(
        shards,
        mesh=split,
        in_specs=(
            P(sp + tp, None),
            P(sp, None),
            P(),
            P(),
            P(None, sp, tp),
            P(None, tp),
            P(None, tp),
            P(None, tp),
            P(tp),
            P(tp),
            P(),
            P(tp, None),
        ),
        out_specs=P(sp + tp, None),
        check_vma=False,
    )
```

```python
import functools
import math

import jax
import jax.numpy as jnp
import numpy as np
from jax import lax
from jax.experimental import pallas as pl
from jax.experimental.pallas import tpu as pltpu
from jax.sharding import Mesh
from jax.sharding import PartitionSpec as P

MESH = pl.DeviceIdType.MESH
F32 = jnp.float32
BF16 = jnp.bfloat16
GRID_W = 64
EPS = 1e-5
NZ = 8
NS = 16
D = 4096
HD = 256
PART = 128
ROWS = 32
LOG2E = math.log2(math.e)
ORDER = (0, 7, 1, 6, 2, 5, 3, 4)
PLACE = {rel: i for i, rel in enumerate(ORDER)}
UNIT = 2 * ROWS
SLOTS_AHEAD = (0, 0, 2, 3, 4, 5)
BLOCK = NZ * UNIT
ANY = pl.BlockSpec(memory_space=pl.ANY)
VM = pl.BlockSpec(memory_space=pltpu.VMEM)
SM = pl.BlockSpec(memory_space=pltpu.SMEM)


def position():
    return tuple(lax.axis_index(a) for a in ("y", "x", "z", "c"))


def sp_peer(i):
    y, x, z, c = position()
    peer = lax.rem(y * 4 + x + i, NS)
    return (peer // 4, lax.rem(peer, 4), z, c)


def tp_peer(i):
    y, x, z, c = position()
    peer = lax.rem(z * 2 + c + i, NS)
    return (y, x, peer // 2, lax.rem(peer, 2))


def greet(peers):
    barrier = pltpu.get_barrier_semaphore()
    for peer_of in peers:

        def one(i, carry):
            pl.semaphore_signal(barrier, inc=1, device_id=peer_of(i), device_id_type=MESH)
            return carry

        lax.fori_loop(1, NS, one, 0)


    y, x, z, c = position()
    pl.semaphore_signal(barrier, inc=1, device_id=(y, 3 - x, z, 1 - c), device_id_type=MESH)


def greeted(peers):
    pl.semaphore_wait(pltpu.get_barrier_semaphore(), (NS - 1) * len(peers) + 1)


def send(src, dst, send_sem, recv_sem, to):
    pltpu.make_async_remote_copy(
        src_ref=src, dst_ref=dst, send_sem=send_sem, recv_sem=recv_sem, device_id=to, device_id_type=MESH
    ).start()


def await_bytes(ref, sem):
    pltpu.make_async_copy(ref, ref, sem).wait()


def silu(v):
    return v / (1.0 + jnp.exp(-v))


def modulated(tokens, shift, scale):
    values = tokens.astype(F32)
    center = jnp.mean(values, axis=-1, keepdims=True)
    values = values - center
    spread = jnp.mean(values * values, axis=-1, keepdims=True)
    return (values * lax.rsqrt(spread + EPS) * (1.0 + scale) + shift).astype(BF16)


def turned(raw, cos, sin):
    lane = lax.broadcasted_iota(jnp.int32, raw.shape, 1)
    partner = jnp.where(lax.rem(lane, 64) < 32, pltpu.roll(raw, HD - 32, 1), pltpu.roll(raw, 32, 1))
    return (raw * cos + partner * sin).astype(BF16)


def tables():
    inverse = 10000.0 ** (-np.arange(32, dtype=np.float32) / np.float32(32))
    inverse = inverse.astype(np.float32)
    row = (np.arange(128, dtype=np.float32)[:, None] * inverse).astype(np.float32).astype(np.float64)
    col = row[:GRID_W]
    zr, zc = np.zeros((128, 64)), np.zeros((GRID_W, 64))

    def lanes(first, second):
        return np.tile(np.concatenate([first, second], axis=1), (1, 2)).astype(np.float32)

    both = lambda a, b: np.concatenate([a, b], axis=1)
    return (
        lanes(both(np.cos(row), np.cos(row)), zr),
        lanes(both(-np.sin(row), np.sin(row)), zr),
        lanes(zc, both(np.cos(col), np.cos(col))),
        lanes(zc, both(-np.sin(col), np.sin(col))),
    )


def front(
    latent, context, cond, ctx_cond, modulation, wq, wk, wv, rcos, rsin, ccos, csin,
    q, kv, ctx, kv_away, ctx_away, mods, ahead, early,
    lat, wq_v, wk_v, wv_v, mod_v, ctx_v, parts, normed,
    load, mod_send, mod_recv, ring_send, ring_recv, pair_send, pair_recv,
):
    y, x, z, c = position()
    sp, tp = y * 4 + x, z * 2 + c
    right = c == x // 2
    seat = lax.rem(x, 2) * 4 + y
    loads = [
        pltpu.make_async_copy(latent, lat.at[z, c], load.at[0]),
        pltpu.make_async_copy(modulation, mod_v, load.at[1]),
        pltpu.make_async_copy(context, ctx_v, load.at[2]),
        pltpu.make_async_copy(wq, wq_v, load.at[3]),
        pltpu.make_async_copy(wk, wk_v, load.at[4]),
        pltpu.make_async_copy(wv, wv_v, load.at[5]),
    ]
    for copy in loads:
        copy.start()

    def half_of(step, way):
        return (0, 1) if step < 4 else ((0,) if way > 0 else (1,))

    def block(rel):
        return lax.rem(z + rel, NZ)

    def ring_step(step, way, half):
        held = block((-way * (step - 1)) % NZ)
        there = (-way * step) % NZ
        rows = pl.ds(half * 16, 16)
        send(
            lat.at[held, c, rows], lat.at[held, c, rows], ring_send.at[there * 2 + half],
            ring_recv.at[there * 2 + half], (y, x, lax.rem(z + way + NZ, NZ), c),
        )

    def ring_wait(rel, half):
        await_bytes(lat.at[block(rel), c, pl.ds(half * 16, 16)], ring_recv.at[rel * 2 + half])

    def pair_step(rel):
        mine = lat.at[block(rel), c]
        send(mine, mine, pair_send.at[rel], pair_recv.at[rel], (y, x, z, 1 - c))

    def pair_wait(rel):
        await_bytes(lat.at[block(rel), 1 - c], pair_recv.at[rel])

    loads[0].wait()
    greeted((sp_peer, tp_peer))
    early()
    for half in (0, 1):
        for way in (1, -1):
            ring_step(1, way, half)
    pair_step(0)

    pick = lax.broadcasted_iota(jnp.int32, (8, PART), 0) == 0
    rows = []
    for j in range(2):
        at = pl.ds(sp * 2 + j, 1)
        rows.append(silu(jnp.where(pick, cond[at, :], ctx_cond[at, :])).astype(BF16))
    loads[1].wait()
    for r in range(3):
        product = jnp.dot(rows[0], mod_v[r, 0:PART], preferred_element_type=F32) + jnp.dot(
            rows[1], mod_v[r, PART : 2 * PART], preferred_element_type=F32
        )
        parts[sp, r : r + 1, :] = product[0:1]
        parts[sp, 3 + r : 4 + r, :] = product[1:2]
    parts[sp, 6:8, :] = jnp.zeros((2, HD), F32)

    def show_part(i, carry):
        send(parts.at[sp], parts.at[sp], mod_send.at[0], mod_recv.at[0], sp_peer(i))
        return carry

    lax.fori_loop(1, NS, show_part, 0)
    await_bytes(parts.at[pl.ds(0, NS - 1)], mod_recv.at[0])
    total = parts[0]
    for i in range(1, NS):
        total = total + parts[i]
    own_cols = pl.ds(pl.multiple_of(tp * HD, HD), HD)
    mods[:, own_cols] = total

    def show_sum(i, carry):
        send(mods.at[:, own_cols], mods.at[:, own_cols], mod_send.at[1], mod_recv.at[1], tp_peer(i))
        return carry

    lax.fori_loop(1, NS, show_sum, 0)

    def forward(step):
        for half in (0, 1):
            for way in (1, -1):
                ring_wait((-way * step) % NZ, half)
                if half in half_of(step + 1, way):
                    ring_step(step + 1, way, half)
        for way in (1, -1):
            pair_step((-way * step) % NZ)

    def norm_rows(load_rows, where, pick_mod):
        shift, scale = mods[pick_mod : pick_mod + 1, :], mods[pick_mod + 1 : pick_mod + 2, :]
        for half in (0, 1):
            normed[where + half * 16 : where + half * 16 + 16, :] = modulated(
                load_rows(pl.ds(half * 16, 16)), shift, scale
            )

    def project(units, with_context):
        count = len(units)
        for i, rel in enumerate(units):
            zz = block(rel)
            for core in (0, 1):
                norm_rows(lambda rows, zz=zz, core=core: lat[zz, core, rows, :], i * UNIT + core * ROWS, 0)
        if with_context:
            norm_rows(lambda rows: ctx_v[rows, :], count * UNIT, 3)
        end = count * UNIT + (ROWS if with_context else 0)
        lhs = normed[0:end, :]
        q_raw = jnp.dot(lhs, wq_v[...], preferred_element_type=F32).astype(BF16)
        k_raw = jnp.dot(lhs, wk_v[...], preferred_element_type=F32).astype(BF16)
        v_raw = jnp.dot(lhs, wv_v[...], preferred_element_type=F32).astype(BF16)
        for i, rel in enumerate(units):
            o = PLACE[rel]
            line = pl.ds(sp * NZ + block(rel), 1)
            cos = rcos[line, :] + ccos[...]
            sin = rsin[line, :] + csin[...]
            part = slice(i * UNIT, (i + 1) * UNIT)
            q[0, o * UNIT : (o + 1) * UNIT, :] = turned(q_raw[part].astype(F32), cos, sin)
            keys = turned(k_raw[part].astype(F32), cos, sin)

            @pl.when(right)
            def _():
                here = pl.ds(pl.multiple_of(seat * UNIT, UNIT), UNIT)
                kv[c, o, here, 0:HD] = keys
                kv[c, o, here, HD : 2 * HD] = v_raw[part]

            @pl.when(jnp.logical_not(right))
            def _():
                kv_away[o, :, 0:HD] = keys
                kv_away[o, :, HD : 2 * HD] = v_raw[part]

        if with_context:

            @pl.when(right)
            def _():
                here = pl.ds(pl.multiple_of(seat * ROWS, ROWS), ROWS)
                ctx[c, 0, here, 0:HD] = k_raw[count * UNIT : end]
                ctx[c, 0, here, HD : 2 * HD] = v_raw[count * UNIT : end]

            @pl.when(jnp.logical_not(right))
            def _():
                ctx_away[:, 0:HD] = k_raw[count * UNIT : end]
                ctx_away[:, HD : 2 * HD] = v_raw[count * UNIT : end]

    forward(1)
    forward(2)
    await_bytes(mods.at[:, pl.ds(0, (NS - 1) * HD)], mod_recv.at[1])
    for copy in loads[2:]:
        copy.wait()
    pair_wait(0)
    project([0], True)
    ahead(0)
    for rel in (7, 1):
        pair_wait(rel)
    project([7, 1], False)
    ahead(1)
    forward(3)
    for rel in (6, 2):
        pair_wait(rel)
    project([6, 2], False)
    ahead(2)
    ring_wait(4, 0)
    ring_wait(4, 1)
    pair_step(4)
    for rel in (5, 3):
        pair_wait(rel)
    project([5, 3], False)
    ahead(3)
    pair_wait(4)
    project([4], False)
    ahead(4)

    await_bytes(parts.at[pl.ds(0, NS - 1)], mod_send.at[0])
    await_bytes(mods.at[:, pl.ds(0, (NS - 1) * HD)], mod_send.at[1])
    for i in range(2, 2 * NZ):
        await_bytes(lat.at[0, 0, pl.ds(0, 16)], ring_send.at[i])
    for rel in range(NZ):
        await_bytes(lat.at[0, 0], pair_send.at[rel])


def gather_unit(kv, tall, kv_send, kv_recv):
    y, x, z, c = position()
    mate = x + 1 - 2 * lax.rem(x, 2)

    def wrap(v):
        return lax.rem(v + 8, 4)

    def way_of(o):
        return 1 - 2 * lax.rem(o // 2, 2)

    def step(o, crossed, dy, over, ty, kind):
        ox = mate if crossed else x
        seat = lax.rem(ox, 2) * 4 + wrap(y + dy)
        rows = pl.ds(pl.multiple_of(seat * tall, tall), tall)
        send(
            kv.at[c, o, rows], kv.at[c, o, rows], kv_send.at[0], kv_recv.at[o * 4 + kind],
            (wrap(y + ty), mate if over else x, z, c),
        )

    def wait(o, kind, count=1):
        await_bytes(kv.at[c, o, pl.ds(0, count * tall)], kv_recv.at[o * 4 + kind])

    def typed(o, even, odd):
        if isinstance(o, int):
            (odd if o % 2 else even)()
        else:
            pl.when(lax.rem(o, 2) == 0)(even)
            pl.when(lax.rem(o, 2) == 1)(odd)

    def own(o):
        way = way_of(o)

        def even():
            step(o, False, 0, True, 0, 0)
            step(o, False, 0, False, way, 1)
            step(o, False, 0, False, -way, 3)

        def odd():
            step(o, False, 0, False, way, 1)
            step(o, False, 0, False, -way, 0)
            step(o, False, 0, True, 0, 3)

        typed(o, even, odd)

    def stage1(o):
        way = way_of(o)

        def even():
            wait(o, 0)
            step(o, True, 0, False, way, 2)
            step(o, True, 0, False, -way, 3)

        def odd():
            wait(o, 1)
            step(o, False, -way, False, way, 2)
            step(o, False, -way, True, 0, 3)
            wait(o, 0)
            step(o, False, way, True, 0, 3)

        typed(o, even, odd)

    def stage2(o):
        way = way_of(o)

        def even():
            wait(o, 1)
            step(o, False, -way, False, way, 3)

        def odd():
            wait(o, 2)
            step(o, False, 2, True, 0, 3)

        typed(o, even, odd)

    def stage3(o):
        way = way_of(o)

        def even():
            wait(o, 2)
            step(o, True, -way, False, way, 3)

        typed(o, even, lambda: None)

    def done(o):
        wait(o, 3, 4)

    def all_sent(units):
        for o in range(units):
            await_bytes(kv.at[0, 0, pl.ds(0, 7 * tall)], kv_send.at[0])

    return own, (stage1, stage2, stage3), done, all_sent


def absorb(q, slot, rows, keys, values, lift, peak, sums, acc):
    for m in range(2):
        scores = lax.dot_general(
            q[slot, rows, m * PART : (m + 1) * PART], keys(m), (((1,), (1,)), ((), ())), preferred_element_type=F32
        )
        scores = scores * (PART**-0.5 * LOG2E)
        if lift is not None:
            scores = scores + lift
        before = peak[m, rows]
        now = jnp.maximum(before, jnp.max(scores, axis=1, keepdims=True))
        fading = jnp.exp2(before - now)
        weights = jnp.exp2(scores - now[:, 0:1])
        sums[m, rows] = sums[m, rows] * fading + jnp.sum(weights, axis=1, keepdims=True)
        acc[m, rows] = acc[m, rows] * fading[:, 0:1] + jnp.dot(
            weights.astype(BF16), values(), preferred_element_type=F32
        )
        peak[m, rows] = now


CHUNKS = 4
WIDE = D // CHUNKS


def back(
    heads, lat, mods,
    result,
    wo_v, wo_pair, part, out_buf, in_buf,
    pair_send, pair_recv, out_send, out_recv,
):
    y, x, z, c = position()
    mine, theirs = heads[0], heads[1]
    await_bytes(wo_pair, pair_recv.at[1])

    def long_way(j):
        return 0 if j < 2 else 1

    def slot(way, step, j):
        return (way * 4 + step - 1) * CHUNKS + j

    def hop(way, step, j, add):
        rel = (5 - step) if way == 0 else (3 + step) % NZ
        value = part[j, PLACE[rel]]
        if add:
            value = value + in_buf[slot(way, step - 1, j)].astype(F32)
        s = slot(way, step, j)
        out_buf[s] = value.astype(BF16)
        to = lax.rem(z + (1 if way == 0 else NZ - 1), NZ)
        send(out_buf.at[s], in_buf.at[s], out_send.at[s], out_recv.at[s], (y, x, to, c))

    def hop_wait(way, step, j):
        s = slot(way, step, j)
        await_bytes(in_buf.at[s], out_recv.at[s])

    for j in (0, 2, 1, 3):
        cols = slice(j * WIDE, (j + 1) * WIDE)
        product = jnp.dot(mine, wo_v[:, cols], preferred_element_type=F32) + jnp.dot(
            theirs, wo_pair[:, cols], preferred_element_type=F32
        )
        part[j] = product.reshape(NZ, ROWS, WIDE)
        hop(long_way(j), 1, j, False)
    for j in (0, 2, 1, 3):
        hop(1 - long_way(j), 2, j, False)
    for step in (1, 2, 3):
        if step > 1:
            for j in (0, 2, 1, 3):
                way = 1 - long_way(j)
                hop_wait(way, step, j)
                hop(way, step + 1, j, True)
        for j in (0, 2, 1, 3):
            way = long_way(j)
            hop_wait(way, step, j)
            hop(way, step + 1, j, True)
    for j in (0, 2, 1, 3):
        cols = slice(j * WIDE, (j + 1) * WIDE)
        total = part[j, 0]
        for way in (1 - long_way(j), long_way(j)):
            hop_wait(way, 4, j)
            total = total + in_buf[slot(way, 4, j)].astype(F32)
        result[:, cols] = (lat[z, c, :, cols].astype(F32) + mods[2:3, cols] * total).astype(BF16)
    await_bytes(wo_pair, pair_send.at[1])
    for way in (0, 1):
        for step in (1, 2, 3, 4):
            for j in range(CHUNKS):
                if step > 1 or long_way(j) == way:
                    s = slot(way, step, j)
                    await_bytes(out_buf.at[s], out_send.at[s])


def kernel(
    latent, context, cond, ctx_cond, modulation, wq, wk, wv, rcos, rsin, ccos, csin, lift, lam, gain, wo,
    result,
    lat, wq_v, wk_v, wv_v, mod_v, ctx_v, parts, normed, mods,
    q, kv, ctx, kv_away, ctx_away, settings, peak, sums, acc, attended, heads,
    wo_v, wo_pair, part, out_buf, in_buf,
    load, mod_send, mod_recv, ring_send, ring_recv, pair_send, pair_recv,
    kv_send, kv_recv, ctx_send, ctx_recv, away_send, away_recv, lane_send, lane_recv, set_send, set_recv,
    head_send, head_recv, back_load, back_send, back_recv, out_send, out_recv,
):
    y, x, z, c = position()
    greet((sp_peer, tp_peer))
    group = x // 2
    right = c == group
    wrong = c != group
    partner = (y, 3 - x, z, 1 - c)
    sibling = (y, x, z, 1 - c)
    wo_copy = pltpu.make_async_copy(wo, wo_v, back_load.at[0])
    own, stages, done, all_sent = gather_unit(kv, UNIT, kv_send, kv_recv)
    ctx_own, ctx_stages, ctx_done, ctx_all_sent = gather_unit(ctx, ROWS, ctx_send, ctx_recv)
    settings[0, 0] = jnp.full((8, 128), lift[0] * LOG2E, F32)
    settings[0, 1] = jnp.full((8, 128), lam[0], F32)
    peak[...] = jnp.full(peak.shape, -jnp.inf, F32)
    sums[...] = jnp.zeros(sums.shape, F32)
    acc[...] = jnp.zeros(acc.shape, F32)
    there = lax.rem(3 - x, 2) * 4 + y
    here = lax.rem(x, 2) * 4 + y

    def early():
        send(settings.at[0], settings.at[1], set_send.at[0], set_recv.at[0], sibling)

    def away(*units):
        @pl.when(wrong)
        def _():
            for o in units:
                rows = pl.ds(o * UNIT, UNIT)
                send(q.at[0, rows], q.at[1, rows], away_send.at[0], away_recv.at[NZ + 1], partner)
                send(
                    kv_away.at[o], kv.at[1 - c, o, pl.ds(pl.multiple_of(there * UNIT, UNIT), UNIT)],
                    away_send.at[1], away_recv.at[o], partner,
                )

    def ctx_away_start():
        @pl.when(wrong)
        def _():
            send(
                ctx_away, ctx.at[1 - c, 0, pl.ds(pl.multiple_of(there * ROWS, ROWS), ROWS)],
                away_send.at[2], away_recv.at[NZ], partner,
            )

    def begin(o):
        @pl.when(wrong)
        def _():
            await_bytes(kv.at[0, 0, pl.ds(0, UNIT)], away_recv.at[o])

        own(o)

    def ctx_begin(o):
        @pl.when(wrong)
        def _():
            await_bytes(ctx.at[0, 0, pl.ds(0, ROWS)], away_recv.at[NZ])

        ctx_own(o)

    def show_lane(o):
        done(o)
        send(kv.at[c, o], kv.at[c, o], lane_send.at[0], lane_recv.at[o], sibling)

    def ctx_show_lane(o):
        ctx_done(o)
        send(ctx.at[c], ctx.at[c], lane_send.at[1], lane_recv.at[NZ], sibling)

    choice = jnp.where(right, 0, 1)

    half = BLOCK // 2

    def attend(r):
        rows = slice(r * half, (r + 1) * half)

        def one(o):
            if r == 0:
                await_bytes(kv.at[0, 0], lane_recv.at[o])
            absorb(
                q, choice, rows,
                lambda m: kv[:, o, :, m * PART : (m + 1) * PART].reshape(NS * UNIT, PART),
                lambda: kv[:, o, :, HD : 2 * HD].reshape(NS * UNIT, HD), None, peak, sums, acc,
            )
            pl.when(o == NZ - 1)(functools.partial(finish, r))

        return one

    def ctx_attend(o):
        await_bytes(ctx.at[0], lane_recv.at[NZ])
        lift_term = settings[choice, 0, 0:1, 0:1]
        for r in range(2):
            absorb(
                q, choice, slice(r * half, (r + 1) * half),
                lambda m: ctx[:, 0, :, m * PART : (m + 1) * PART].reshape(NS * ROWS, PART),
                lambda: ctx[:, 0, :, HD : 2 * HD].reshape(NS * ROWS, HD), lift_term, peak, sums, acc,
            )

    def finish(r):
        rows = slice(r * half, (r + 1) * half)
        means = [acc[m, rows] / sums[m, rows][:, 0:1] for m in range(2)]
        difference = means[0] - settings[choice, 1, 0:1, 0:1] * means[1]
        spread = jnp.mean(difference * difference, axis=1, keepdims=True)
        final = (difference * lax.rsqrt(spread + EPS) * gain[...]).astype(BF16).reshape(NZ // 2, 2, ROWS, HD)
        ours = slice(r * half // 2, (r + 1) * half // 2)
        for core in (0, 1):
            attended[core, ours] = final[:, core].reshape(half // 2, HD)

        @pl.when(right)
        def _():
            heads[0, ours] = attended[c, ours]
            send(attended.at[1 - c, ours], heads.at[1, ours], head_send.at[2 * r], head_recv.at[r], sibling)

        @pl.when(wrong)
        def _():
            for core in (0, 1):
                slot = jnp.where(c == core, 1, 0)
                send(
                    attended.at[core, ours], heads.at[slot, ours], head_send.at[2 * r + core], head_recv.at[2 + r],
                    (y, 3 - x, z, core),
                )

    steps = (
        (3, stages[2]), (0, begin), (5, attend(0)), (4, show_lane), (1, stages[0]), (2, stages[1]), (5, attend(1)),
    )
    ctx_steps = {
        1: ctx_begin, 2: ctx_stages[0], 3: ctx_stages[1], 4: ctx_stages[2], 5: ctx_show_lane, 6: ctx_attend,
    }

    def slot(t):
        for after, one in steps:
            o = t - after
            if isinstance(t, int):
                if 0 <= o < NZ:
                    one(o)
            else:

                @pl.when((o >= 0) & (o < NZ))
                def _(o=o, one=one):
                    one(o)

        for at, one in ctx_steps.items():
            if isinstance(t, int):
                if t == at:
                    one(0)
            elif at >= SLOTS_AHEAD[-1]:

                @pl.when(t == at)
                def _(one=one):
                    one(0)

    def ahead(step):
        if step == 0:
            away(0)
            ctx_away_start()
            wo_copy.start()
        else:
            away(*((2 * step - 1, 2 * step) if step < 4 else (7,)))
        for t in range(SLOTS_AHEAD[step], SLOTS_AHEAD[step + 1]):
            slot(t)
        if step == 1:
            wo_copy.wait()
            send(wo_v, wo_pair, back_send.at[1], back_recv.at[1], sibling)

    front(
        latent, context, cond, ctx_cond, modulation, wq, wk, wv, rcos, rsin, ccos, csin,
        q, kv, ctx, kv_away, ctx_away, mods, ahead, early,
        lat, wq_v, wk_v, wv_v, mod_v, ctx_v, parts, normed,
        load, mod_send, mod_recv, ring_send, ring_recv, pair_send, pair_recv,
    )
    await_bytes(settings.at[1], set_recv.at[0])

    @pl.when(wrong)
    def _():
        await_bytes(q.at[1], away_recv.at[NZ + 1])

    def later(t, carry):
        slot(t)
        return carry

    lax.fori_loop(SLOTS_AHEAD[-1], NZ + 5, later, 0)
    some = heads.at[0, pl.ds(0, half // 2)]
    for r in range(2):
        await_bytes(some, head_recv.at[2 + r])

        @pl.when(wrong)
        def _(r=r):
            await_bytes(some, head_recv.at[r])

    back(
        heads, lat, mods, result, wo_v, wo_pair, part, out_buf, in_buf,
        back_send, back_recv, out_send, out_recv,
    )
    all_sent(NZ)
    ctx_all_sent(1)
    await_bytes(settings.at[0], set_send.at[0])
    await_bytes(ctx.at[0], lane_send.at[1])
    for o in range(NZ):
        await_bytes(kv.at[0, 0], lane_send.at[0])
    for r in range(2):
        await_bytes(some, head_send.at[2 * r])

    @pl.when(wrong)
    def _():
        for r in range(2):
            await_bytes(some, head_send.at[2 * r + 1])
        await_bytes(q.at[0], away_send.at[0])
        await_bytes(kv_away, away_send.at[1])
        await_bytes(ctx_away, away_send.at[2])


def run(*arrays):
    dma = pltpu.SemaphoreType.DMA
    slots = 2 * 4 * CHUNKS
    return pl.pallas_call(
        kernel,
        out_shape=jax.ShapeDtypeStruct((ROWS, D), BF16),
        in_specs=[ANY, ANY, VM, VM, ANY, ANY, ANY, ANY, VM, VM, VM, VM, SM, SM, VM, ANY],
        out_specs=VM,
        scratch_shapes=[
            pltpu.VMEM((NZ, 2, ROWS, D), BF16),
            pltpu.VMEM((D, HD), BF16),
            pltpu.VMEM((D, HD), BF16),
            pltpu.VMEM((D, HD), BF16),
            pltpu.VMEM((3, HD, HD), BF16),
            pltpu.VMEM((ROWS, D), BF16),
            pltpu.VMEM((NS, 8, HD), F32),
            pltpu.VMEM((2 * UNIT, D), BF16),
            pltpu.VMEM((8, D), F32),
            pltpu.VMEM((2, BLOCK, HD), BF16),
            pltpu.VMEM((2, NZ, NS // 2 * UNIT, 2 * HD), BF16),
            pltpu.VMEM((2, 1, NS // 2 * ROWS, 2 * HD), BF16),
            pltpu.VMEM((NZ, UNIT, 2 * HD), BF16),
            pltpu.VMEM((ROWS, 2 * HD), BF16),
            pltpu.VMEM((2, 2, 8, 128), F32),
            pltpu.VMEM((2, BLOCK, 128), F32),
            pltpu.VMEM((2, BLOCK, 128), F32),
            pltpu.VMEM((2, BLOCK, HD), F32),
            pltpu.VMEM((2, HD, HD), BF16),
            pltpu.VMEM((2, HD, HD), BF16),
            pltpu.VMEM((HD, D), BF16),
            pltpu.VMEM((HD, D), BF16),
            pltpu.VMEM((CHUNKS, NZ, ROWS, WIDE), F32),
            pltpu.VMEM((slots, ROWS, WIDE), BF16),
            pltpu.VMEM((slots, ROWS, WIDE), BF16),
            dma((6,)),
            dma((2,)),
            dma((2,)),
            dma((2 * NZ,)),
            dma((2 * NZ,)),
            dma((NZ,)),
            dma((NZ,)),
            dma((1,)),
            dma((4 * NZ,)),
            dma((1,)),
            dma((4,)),
            dma((3,)),
            dma((NZ + 2,)),
            dma((2,)),
            dma((NZ + 1,)),
            dma((1,)),
            dma((1,)),
            dma((4,)),
            dma((4,)),
            dma((1,)),
            dma((2,)),
            dma((2,)),
            dma((slots,)),
            dma((slots,)),
        ],
        compiler_params=pltpu.CompilerParams(
            collective_id=0, has_side_effects=True, vmem_limit_bytes=60 * 2**20
        ),
        name="whole",
    )(*arrays)


def shards(
    latent, context, condition, context_condition, modulation,
    query_weight, key_weight, value_weight, lambdas, context_lift, head_gain, output_weight,
):
    return run(
        latent, context, condition.reshape(32, 128), context_condition.reshape(32, 128),
        modulation, query_weight, key_weight, value_weight, *[jnp.asarray(t) for t in tables()],
        context_lift, lambdas, head_gain.reshape(1, HD), output_weight,
    )


def solution(mesh):
    split = Mesh(mesh.devices.reshape(4, 4, NZ, 2), ("y", "x", "z", "c"))
    sp, tp = ("y", "x"), ("z", "c")
    return jax.shard_map(
        shards,
        mesh=split,
        in_specs=(
            P(sp + tp, None),
            P(sp, None),
            P(),
            P(),
            P(None, sp, tp),
            P(None, tp),
            P(None, tp),
            P(None, tp),
            P(tp),
            P(tp),
            P(),
            P(tp, None),
        ),
        out_specs=P(sp + tp, None),
        check_vma=False,
    )
```

```python
import functools
import math

import jax
import jax.numpy as jnp
import numpy as np
from jax import lax
from jax.experimental import pallas as pl
from jax.experimental.pallas import tpu as pltpu
from jax.sharding import Mesh
from jax.sharding import PartitionSpec as P

MESH = pl.DeviceIdType.MESH
F32 = jnp.float32
BF16 = jnp.bfloat16
GRID_W = 64
EPS = 1e-5
NZ = 8
NS = 16
D = 4096
HD = 256
PART = 128
ROWS = 32
LOG2E = math.log2(math.e)
ORDER = (0, 7, 1, 6, 2, 5, 3, 4)
PLACE = {rel: i for i, rel in enumerate(ORDER)}
UNIT = 2 * ROWS
SLOTS_AHEAD = (0, 0, 2, 3, 4, 5)
BLOCK = NZ * UNIT
ANY = pl.BlockSpec(memory_space=pl.ANY)
VM = pl.BlockSpec(memory_space=pltpu.VMEM)
SM = pl.BlockSpec(memory_space=pltpu.SMEM)


def position():
    return tuple(lax.axis_index(a) for a in ("y", "x", "z", "c"))


def sp_peer(i):
    y, x, z, c = position()
    peer = lax.rem(y * 4 + x + i, NS)
    return (peer // 4, lax.rem(peer, 4), z, c)


def tp_peer(i):
    y, x, z, c = position()
    peer = lax.rem(z * 2 + c + i, NS)
    return (y, x, peer // 2, lax.rem(peer, 2))


def greet(peers):
    barrier = pltpu.get_barrier_semaphore()
    for peer_of in peers:

        def one(i, carry):
            pl.semaphore_signal(barrier, inc=1, device_id=peer_of(i), device_id_type=MESH)
            return carry

        lax.fori_loop(1, NS, one, 0)


    y, x, z, c = position()
    pl.semaphore_signal(barrier, inc=1, device_id=(y, 3 - x, z, 1 - c), device_id_type=MESH)


def greeted(peers):
    pl.semaphore_wait(pltpu.get_barrier_semaphore(), (NS - 1) * len(peers) + 1)


def send(src, dst, send_sem, recv_sem, to):
    pltpu.make_async_remote_copy(
        src_ref=src, dst_ref=dst, send_sem=send_sem, recv_sem=recv_sem, device_id=to, device_id_type=MESH
    ).start()


def await_bytes(ref, sem):
    pltpu.make_async_copy(ref, ref, sem).wait()


def silu(v):
    return v / (1.0 + jnp.exp(-v))


def modulated(tokens, shift, scale):
    values = tokens.astype(F32)
    center = jnp.mean(values, axis=-1, keepdims=True)
    values = values - center
    spread = jnp.mean(values * values, axis=-1, keepdims=True)
    return (values * lax.rsqrt(spread + EPS) * (1.0 + scale) + shift).astype(BF16)


def turned(raw, cos, sin):
    lane = lax.broadcasted_iota(jnp.int32, raw.shape, 1)
    partner = jnp.where(lax.rem(lane, 64) < 32, pltpu.roll(raw, HD - 32, 1), pltpu.roll(raw, 32, 1))
    return (raw * cos + partner * sin).astype(BF16)


def tables():
    inverse = 10000.0 ** (-np.arange(32, dtype=np.float32) / np.float32(32))
    inverse = inverse.astype(np.float32)
    row = (np.arange(128, dtype=np.float32)[:, None] * inverse).astype(np.float32).astype(np.float64)
    col = row[:GRID_W]
    zr, zc = np.zeros((128, 64)), np.zeros((GRID_W, 64))

    def lanes(first, second):
        return np.tile(np.concatenate([first, second], axis=1), (1, 2)).astype(np.float32)

    both = lambda a, b: np.concatenate([a, b], axis=1)
    return (
        lanes(both(np.cos(row), np.cos(row)), zr),
        lanes(both(-np.sin(row), np.sin(row)), zr),
        lanes(zc, both(np.cos(col), np.cos(col))),
        lanes(zc, both(-np.sin(col), np.sin(col))),
    )


def front(
    latent, context, cond, ctx_cond, modulation, wq, wk, wv, rcos, rsin, ccos, csin,
    q, kv, ctx, kv_away, ctx_away, mods, ahead, early,
    lat, wq_v, wk_v, wv_v, mod_v, ctx_v, parts, normed,
    load, mod_send, mod_recv, ring_send, ring_recv, pair_send, pair_recv,
):
    y, x, z, c = position()
    sp, tp = y * 4 + x, z * 2 + c
    right = c == x // 2
    seat = lax.rem(x, 2) * 4 + y
    loads = [
        pltpu.make_async_copy(latent, lat.at[z, c], load.at[0]),
        pltpu.make_async_copy(modulation, mod_v, load.at[1]),
        pltpu.make_async_copy(context, ctx_v, load.at[2]),
        pltpu.make_async_copy(wq, wq_v, load.at[3]),
        pltpu.make_async_copy(wk, wk_v, load.at[4]),
        pltpu.make_async_copy(wv, wv_v, load.at[5]),
    ]
    for copy in loads:
        copy.start()

    def half_of(step, way):
        return (0, 1) if step < 4 else ((0,) if way > 0 else (1,))

    def block(rel):
        return lax.rem(z + rel, NZ)

    def ring_step(step, way, half):
        held = block((-way * (step - 1)) % NZ)
        there = (-way * step) % NZ
        rows = pl.ds(half * 16, 16)
        send(
            lat.at[held, c, rows], lat.at[held, c, rows], ring_send.at[there * 2 + half],
            ring_recv.at[there * 2 + half], (y, x, lax.rem(z + way + NZ, NZ), c),
        )

    def ring_wait(rel, half):
        await_bytes(lat.at[block(rel), c, pl.ds(half * 16, 16)], ring_recv.at[rel * 2 + half])

    def pair_step(rel):
        mine = lat.at[block(rel), c]
        send(mine, mine, pair_send.at[rel], pair_recv.at[rel], (y, x, z, 1 - c))

    def pair_wait(rel):
        await_bytes(lat.at[block(rel), 1 - c], pair_recv.at[rel])

    loads[0].wait()
    greeted((sp_peer, tp_peer))
    early()
    for half in (0, 1):
        for way in (1, -1):
            ring_step(1, way, half)
    pair_step(0)

    pick = lax.broadcasted_iota(jnp.int32, (8, PART), 0) == 0
    rows = []
    for j in range(2):
        at = pl.ds(sp * 2 + j, 1)
        rows.append(silu(jnp.where(pick, cond[at, :], ctx_cond[at, :])).astype(BF16))
    loads[1].wait()
    for r in range(3):
        product = jnp.dot(rows[0], mod_v[r, 0:PART], preferred_element_type=F32) + jnp.dot(
            rows[1], mod_v[r, PART : 2 * PART], preferred_element_type=F32
        )
        parts[sp, r : r + 1, :] = product[0:1]
        parts[sp, 3 + r : 4 + r, :] = product[1:2]
    parts[sp, 6:8, :] = jnp.zeros((2, HD), F32)

    def show_part(i, carry):
        send(parts.at[sp], parts.at[sp], mod_send.at[0], mod_recv.at[0], sp_peer(i))
        return carry

    lax.fori_loop(1, NS, show_part, 0)
    await_bytes(parts.at[pl.ds(0, NS - 1)], mod_recv.at[0])
    total = parts[0]
    for i in range(1, NS):
        total = total + parts[i]
    own_cols = pl.ds(pl.multiple_of(tp * HD, HD), HD)
    mods[:, own_cols] = total

    def show_sum(i, carry):
        send(mods.at[:, own_cols], mods.at[:, own_cols], mod_send.at[1], mod_recv.at[1], tp_peer(i))
        return carry

    lax.fori_loop(1, NS, show_sum, 0)

    def forward(step):
        for half in (0, 1):
            for way in (1, -1):
                ring_wait((-way * step) % NZ, half)
                if half in half_of(step + 1, way):
                    ring_step(step + 1, way, half)
        for way in (1, -1):
            pair_step((-way * step) % NZ)

    def norm_rows(load_rows, where, pick_mod):
        shift, scale = mods[pick_mod : pick_mod + 1, :], mods[pick_mod + 1 : pick_mod + 2, :]
        for half in (0, 1):
            normed[where + half * 16 : where + half * 16 + 16, :] = modulated(
                load_rows(pl.ds(half * 16, 16)), shift, scale
            )

    def project(units, with_context):
        count = len(units)
        for i, rel in enumerate(units):
            zz = block(rel)
            for core in (0, 1):
                norm_rows(lambda rows, zz=zz, core=core: lat[zz, core, rows, :], i * UNIT + core * ROWS, 0)
        if with_context:
            norm_rows(lambda rows: ctx_v[rows, :], count * UNIT, 3)
        end = count * UNIT + (ROWS if with_context else 0)
        lhs = normed[0:end, :]
        q_raw = jnp.dot(lhs, wq_v[...], preferred_element_type=F32).astype(BF16)
        k_raw = jnp.dot(lhs, wk_v[...], preferred_element_type=F32).astype(BF16)
        v_raw = jnp.dot(lhs, wv_v[...], preferred_element_type=F32).astype(BF16)
        for i, rel in enumerate(units):
            o = PLACE[rel]
            line = pl.ds(sp * NZ + block(rel), 1)
            cos = rcos[line, :] + ccos[...]
            sin = rsin[line, :] + csin[...]
            part = slice(i * UNIT, (i + 1) * UNIT)
            q[0, o * UNIT : (o + 1) * UNIT, :] = turned(q_raw[part].astype(F32), cos, sin)
            keys = turned(k_raw[part].astype(F32), cos, sin)

            @pl.when(right)
            def _():
                here = pl.ds(pl.multiple_of(seat * UNIT, UNIT), UNIT)
                kv[c, o, here, 0:HD] = keys
                kv[c, o, here, HD : 2 * HD] = v_raw[part]

            @pl.when(jnp.logical_not(right))
            def _():
                kv_away[o, :, 0:HD] = keys
                kv_away[o, :, HD : 2 * HD] = v_raw[part]

        if with_context:

            @pl.when(right)
            def _():
                here = pl.ds(pl.multiple_of(seat * ROWS, ROWS), ROWS)
                ctx[c, 0, here, 0:HD] = k_raw[count * UNIT : end]
                ctx[c, 0, here, HD : 2 * HD] = v_raw[count * UNIT : end]

            @pl.when(jnp.logical_not(right))
            def _():
                ctx_away[:, 0:HD] = k_raw[count * UNIT : end]
                ctx_away[:, HD : 2 * HD] = v_raw[count * UNIT : end]

    forward(1)
    forward(2)
    await_bytes(mods.at[:, pl.ds(0, (NS - 1) * HD)], mod_recv.at[1])
    for copy in loads[2:]:
        copy.wait()
    pair_wait(0)
    project([0], True)
    ahead(0)
    forward(3)
    for rel in (7, 1):
        pair_wait(rel)
    project([7, 1], False)
    ahead(1)
    for rel in (6, 2):
        pair_wait(rel)
    project([6, 2], False)
    ahead(2)
    ring_wait(4, 0)
    ring_wait(4, 1)
    pair_step(4)
    for rel in (5, 3):
        pair_wait(rel)
    project([5, 3], False)
    ahead(3)
    pair_wait(4)
    project([4], False)
    ahead(4)

    await_bytes(parts.at[pl.ds(0, NS - 1)], mod_send.at[0])
    await_bytes(mods.at[:, pl.ds(0, (NS - 1) * HD)], mod_send.at[1])
    for i in range(2, 2 * NZ):
        await_bytes(lat.at[0, 0, pl.ds(0, 16)], ring_send.at[i])
    for rel in range(NZ):
        await_bytes(lat.at[0, 0], pair_send.at[rel])


def gather_unit(kv, tall, kv_send, kv_recv):
    y, x, z, c = position()
    mate = x + 1 - 2 * lax.rem(x, 2)

    def wrap(v):
        return lax.rem(v + 8, 4)

    def way_of(o):
        return 1 - 2 * lax.rem(o // 2, 2)

    def step(o, crossed, dy, over, ty, kind):
        ox = mate if crossed else x
        seat = lax.rem(ox, 2) * 4 + wrap(y + dy)
        rows = pl.ds(pl.multiple_of(seat * tall, tall), tall)
        send(
            kv.at[c, o, rows], kv.at[c, o, rows], kv_send.at[0], kv_recv.at[o * 4 + kind],
            (wrap(y + ty), mate if over else x, z, c),
        )

    def wait(o, kind, count=1):
        await_bytes(kv.at[c, o, pl.ds(0, count * tall)], kv_recv.at[o * 4 + kind])

    def typed(o, even, odd):
        if isinstance(o, int):
            (odd if o % 2 else even)()
        else:
            pl.when(lax.rem(o, 2) == 0)(even)
            pl.when(lax.rem(o, 2) == 1)(odd)

    def own(o):
        way = way_of(o)

        def even():
            step(o, False, 0, True, 0, 0)
            step(o, False, 0, False, way, 1)
            step(o, False, 0, False, -way, 3)

        def odd():
            step(o, False, 0, False, way, 1)
            step(o, False, 0, False, -way, 0)
            step(o, False, 0, True, 0, 3)

        typed(o, even, odd)

    def stage1(o):
        way = way_of(o)

        def even():
            wait(o, 0)
            step(o, True, 0, False, way, 2)
            step(o, True, 0, False, -way, 3)

        def odd():
            wait(o, 1)
            step(o, False, -way, False, way, 2)
            step(o, False, -way, True, 0, 3)
            wait(o, 0)
            step(o, False, way, True, 0, 3)

        typed(o, even, odd)

    def stage2(o):
        way = way_of(o)

        def even():
            wait(o, 1)
            step(o, False, -way, False, way, 3)

        def odd():
            wait(o, 2)
            step(o, False, 2, True, 0, 3)

        typed(o, even, odd)

    def stage3(o):
        way = way_of(o)

        def even():
            wait(o, 2)
            step(o, True, -way, False, way, 3)

        typed(o, even, lambda: None)

    def done(o):
        wait(o, 3, 4)

    def all_sent(units):
        for o in range(units):
            await_bytes(kv.at[0, 0, pl.ds(0, 7 * tall)], kv_send.at[0])

    return own, (stage1, stage2, stage3), done, all_sent


def absorb(q, slot, rows, keys, values, lift, peak, sums, acc):
    for m in range(2):
        scores = lax.dot_general(
            q[slot, rows, m * PART : (m + 1) * PART], keys(m), (((1,), (1,)), ((), ())), preferred_element_type=F32
        )
        scores = scores * (PART**-0.5 * LOG2E)
        if lift is not None:
            scores = scores + lift
        before = peak[m, rows]
        now = jnp.maximum(before, jnp.max(scores, axis=1, keepdims=True))
        fading = jnp.exp2(before - now)
        weights = jnp.exp2(scores - now[:, 0:1])
        sums[m, rows] = sums[m, rows] * fading + jnp.sum(weights, axis=1, keepdims=True)
        acc[m, rows] = acc[m, rows] * fading[:, 0:1] + jnp.dot(
            weights.astype(BF16), values(), preferred_element_type=F32
        )
        peak[m, rows] = now


CHUNKS = 4
WIDE = D // CHUNKS


def back(
    heads, lat, mods,
    result,
    wo_v, wo_pair, part, out_buf, in_buf,
    pair_send, pair_recv, out_send, out_recv,
):
    y, x, z, c = position()
    mine, theirs = heads[0], heads[1]
    await_bytes(wo_pair, pair_recv.at[1])

    def long_way(j):
        return 0 if j < 2 else 1

    def slot(way, step, j):
        return (way * 4 + step - 1) * CHUNKS + j

    def hop(way, step, j, add):
        rel = (5 - step) if way == 0 else (3 + step) % NZ
        value = part[j, PLACE[rel]]
        if add:
            value = value + in_buf[slot(way, step - 1, j)].astype(F32)
        s = slot(way, step, j)
        out_buf[s] = value.astype(BF16)
        to = lax.rem(z + (1 if way == 0 else NZ - 1), NZ)
        send(out_buf.at[s], in_buf.at[s], out_send.at[s], out_recv.at[s], (y, x, to, c))

    def hop_wait(way, step, j):
        s = slot(way, step, j)
        await_bytes(in_buf.at[s], out_recv.at[s])

    for j in (0, 2, 1, 3):
        cols = slice(j * WIDE, (j + 1) * WIDE)
        product = jnp.dot(mine, wo_v[:, cols], preferred_element_type=F32) + jnp.dot(
            theirs, wo_pair[:, cols], preferred_element_type=F32
        )
        part[j] = product.reshape(NZ, ROWS, WIDE)
        hop(long_way(j), 1, j, False)
    for j in (0, 2, 1, 3):
        hop(1 - long_way(j), 2, j, False)
    for step in (1, 2, 3):
        if step > 1:
            for j in (0, 2, 1, 3):
                way = 1 - long_way(j)
                hop_wait(way, step, j)
                hop(way, step + 1, j, True)
        for j in (0, 2, 1, 3):
            way = long_way(j)
            hop_wait(way, step, j)
            hop(way, step + 1, j, True)
    for j in (0, 2, 1, 3):
        cols = slice(j * WIDE, (j + 1) * WIDE)
        total = part[j, 0]
        for way in (1 - long_way(j), long_way(j)):
            hop_wait(way, 4, j)
            total = total + in_buf[slot(way, 4, j)].astype(F32)
        result[:, cols] = (lat[z, c, :, cols].astype(F32) + mods[2:3, cols] * total).astype(BF16)
    await_bytes(wo_pair, pair_send.at[1])
    for way in (0, 1):
        for step in (1, 2, 3, 4):
            for j in range(CHUNKS):
                if step > 1 or long_way(j) == way:
                    s = slot(way, step, j)
                    await_bytes(out_buf.at[s], out_send.at[s])


def kernel(
    latent, context, cond, ctx_cond, modulation, wq, wk, wv, rcos, rsin, ccos, csin, lift, lam, gain, wo,
    result,
    lat, wq_v, wk_v, wv_v, mod_v, ctx_v, parts, normed, mods,
    q, kv, ctx, kv_away, ctx_away, settings, peak, sums, acc, attended, heads,
    wo_v, wo_pair, part, out_buf, in_buf,
    load, mod_send, mod_recv, ring_send, ring_recv, pair_send, pair_recv,
    kv_send, kv_recv, ctx_send, ctx_recv, away_send, away_recv, lane_send, lane_recv, set_send, set_recv,
    head_send, head_recv, back_load, back_send, back_recv, out_send, out_recv,
):
    y, x, z, c = position()
    greet((sp_peer, tp_peer))
    group = x // 2
    right = c == group
    wrong = c != group
    partner = (y, 3 - x, z, 1 - c)
    sibling = (y, x, z, 1 - c)
    wo_copy = pltpu.make_async_copy(wo, wo_v, back_load.at[0])
    own, stages, done, all_sent = gather_unit(kv, UNIT, kv_send, kv_recv)
    ctx_own, ctx_stages, ctx_done, ctx_all_sent = gather_unit(ctx, ROWS, ctx_send, ctx_recv)
    settings[0, 0] = jnp.full((8, 128), lift[0] * LOG2E, F32)
    settings[0, 1] = jnp.full((8, 128), lam[0], F32)
    peak[...] = jnp.full(peak.shape, -jnp.inf, F32)
    sums[...] = jnp.zeros(sums.shape, F32)
    acc[...] = jnp.zeros(acc.shape, F32)
    there = lax.rem(3 - x, 2) * 4 + y
    here = lax.rem(x, 2) * 4 + y

    def early():
        send(settings.at[0], settings.at[1], set_send.at[0], set_recv.at[0], sibling)

    def away(*units):
        @pl.when(wrong)
        def _():
            for o in units:
                rows = pl.ds(o * UNIT, UNIT)
                send(q.at[0, rows], q.at[1, rows], away_send.at[0], away_recv.at[NZ + 1], partner)
                send(
                    kv_away.at[o], kv.at[1 - c, o, pl.ds(pl.multiple_of(there * UNIT, UNIT), UNIT)],
                    away_send.at[1], away_recv.at[o], partner,
                )

    def ctx_away_start():
        @pl.when(wrong)
        def _():
            send(
                ctx_away, ctx.at[1 - c, 0, pl.ds(pl.multiple_of(there * ROWS, ROWS), ROWS)],
                away_send.at[2], away_recv.at[NZ], partner,
            )

    def begin(o):
        @pl.when(wrong)
        def _():
            await_bytes(kv.at[0, 0, pl.ds(0, UNIT)], away_recv.at[o])

        own(o)

    def ctx_begin(o):
        @pl.when(wrong)
        def _():
            await_bytes(ctx.at[0, 0, pl.ds(0, ROWS)], away_recv.at[NZ])

        ctx_own(o)

    def show_lane(o):
        done(o)
        send(kv.at[c, o], kv.at[c, o], lane_send.at[0], lane_recv.at[o], sibling)

    def ctx_show_lane(o):
        ctx_done(o)
        send(ctx.at[c], ctx.at[c], lane_send.at[1], lane_recv.at[NZ], sibling)

    choice = jnp.where(right, 0, 1)

    half = BLOCK // 2

    def attend(r):
        rows = slice(r * half, (r + 1) * half)

        def one(o):
            if r == 0:
                await_bytes(kv.at[0, 0], lane_recv.at[o])
            absorb(
                q, choice, rows,
                lambda m: kv[:, o, :, m * PART : (m + 1) * PART].reshape(NS * UNIT, PART),
                lambda: kv[:, o, :, HD : 2 * HD].reshape(NS * UNIT, HD), None, peak, sums, acc,
            )
            pl.when(o == NZ - 1)(functools.partial(finish, r))

        return one

    def ctx_attend(o):
        await_bytes(ctx.at[0], lane_recv.at[NZ])
        lift_term = settings[choice, 0, 0:1, 0:1]
        for r in range(2):
            absorb(
                q, choice, slice(r * half, (r + 1) * half),
                lambda m: ctx[:, 0, :, m * PART : (m + 1) * PART].reshape(NS * ROWS, PART),
                lambda: ctx[:, 0, :, HD : 2 * HD].reshape(NS * ROWS, HD), lift_term, peak, sums, acc,
            )

    def finish(r):
        rows = slice(r * half, (r + 1) * half)
        means = [acc[m, rows] / sums[m, rows][:, 0:1] for m in range(2)]
        difference = means[0] - settings[choice, 1, 0:1, 0:1] * means[1]
        spread = jnp.mean(difference * difference, axis=1, keepdims=True)
        final = (difference * lax.rsqrt(spread + EPS) * gain[...]).astype(BF16).reshape(NZ // 2, 2, ROWS, HD)
        ours = slice(r * half // 2, (r + 1) * half // 2)
        for core in (0, 1):
            attended[core, ours] = final[:, core].reshape(half // 2, HD)

        @pl.when(right)
        def _():
            heads[0, ours] = attended[c, ours]
            send(attended.at[1 - c, ours], heads.at[1, ours], head_send.at[2 * r], head_recv.at[r], sibling)

        @pl.when(wrong)
        def _():
            for core in (0, 1):
                slot = jnp.where(c == core, 1, 0)
                send(
                    attended.at[core, ours], heads.at[slot, ours], head_send.at[2 * r + core], head_recv.at[2 + r],
                    (y, 3 - x, z, core),
                )

    steps = (
        (3, stages[2]), (0, begin), (5, attend(0)), (4, show_lane), (1, stages[0]), (2, stages[1]), (5, attend(1)),
    )
    ctx_steps = {
        1: ctx_begin, 2: ctx_stages[0], 3: ctx_stages[1], 4: ctx_stages[2], 5: ctx_show_lane, 6: ctx_attend,
    }

    def slot(t):
        for after, one in steps:
            o = t - after
            if isinstance(t, int):
                if 0 <= o < NZ:
                    one(o)
            else:

                @pl.when((o >= 0) & (o < NZ))
                def _(o=o, one=one):
                    one(o)

        for at, one in ctx_steps.items():
            if isinstance(t, int):
                if t == at:
                    one(0)
            elif at >= SLOTS_AHEAD[-1]:

                @pl.when(t == at)
                def _(one=one):
                    one(0)

    def ahead(step):
        if step == 0:
            away(0)
            ctx_away_start()
            wo_copy.start()
        else:
            away(*((2 * step - 1, 2 * step) if step < 4 else (7,)))
        for t in range(SLOTS_AHEAD[step], SLOTS_AHEAD[step + 1]):
            slot(t)
        if step == 1:
            wo_copy.wait()
            send(wo_v, wo_pair, back_send.at[1], back_recv.at[1], sibling)

    front(
        latent, context, cond, ctx_cond, modulation, wq, wk, wv, rcos, rsin, ccos, csin,
        q, kv, ctx, kv_away, ctx_away, mods, ahead, early,
        lat, wq_v, wk_v, wv_v, mod_v, ctx_v, parts, normed,
        load, mod_send, mod_recv, ring_send, ring_recv, pair_send, pair_recv,
    )
    await_bytes(settings.at[1], set_recv.at[0])

    @pl.when(wrong)
    def _():
        await_bytes(q.at[1], away_recv.at[NZ + 1])

    def later(t, carry):
        slot(t)
        return carry

    lax.fori_loop(SLOTS_AHEAD[-1], NZ + 5, later, 0)
    some = heads.at[0, pl.ds(0, half // 2)]
    for r in range(2):
        await_bytes(some, head_recv.at[2 + r])

        @pl.when(wrong)
        def _(r=r):
            await_bytes(some, head_recv.at[r])

    back(
        heads, lat, mods, result, wo_v, wo_pair, part, out_buf, in_buf,
        back_send, back_recv, out_send, out_recv,
    )
    all_sent(NZ)
    ctx_all_sent(1)
    await_bytes(settings.at[0], set_send.at[0])
    await_bytes(ctx.at[0], lane_send.at[1])
    for o in range(NZ):
        await_bytes(kv.at[0, 0], lane_send.at[0])
    for r in range(2):
        await_bytes(some, head_send.at[2 * r])

    @pl.when(wrong)
    def _():
        for r in range(2):
            await_bytes(some, head_send.at[2 * r + 1])
        await_bytes(q.at[0], away_send.at[0])
        await_bytes(kv_away, away_send.at[1])
        await_bytes(ctx_away, away_send.at[2])


def run(*arrays):
    dma = pltpu.SemaphoreType.DMA
    slots = 2 * 4 * CHUNKS
    return pl.pallas_call(
        kernel,
        out_shape=jax.ShapeDtypeStruct((ROWS, D), BF16),
        in_specs=[ANY, ANY, VM, VM, ANY, ANY, ANY, ANY, VM, VM, VM, VM, SM, SM, VM, ANY],
        out_specs=VM,
        scratch_shapes=[
            pltpu.VMEM((NZ, 2, ROWS, D), BF16),
            pltpu.VMEM((D, HD), BF16),
            pltpu.VMEM((D, HD), BF16),
            pltpu.VMEM((D, HD), BF16),
            pltpu.VMEM((3, HD, HD), BF16),
            pltpu.VMEM((ROWS, D), BF16),
            pltpu.VMEM((NS, 8, HD), F32),
            pltpu.VMEM((2 * UNIT, D), BF16),
            pltpu.VMEM((8, D), F32),
            pltpu.VMEM((2, BLOCK, HD), BF16),
            pltpu.VMEM((2, NZ, NS // 2 * UNIT, 2 * HD), BF16),
            pltpu.VMEM((2, 1, NS // 2 * ROWS, 2 * HD), BF16),
            pltpu.VMEM((NZ, UNIT, 2 * HD), BF16),
            pltpu.VMEM((ROWS, 2 * HD), BF16),
            pltpu.VMEM((2, 2, 8, 128), F32),
            pltpu.VMEM((2, BLOCK, 128), F32),
            pltpu.VMEM((2, BLOCK, 128), F32),
            pltpu.VMEM((2, BLOCK, HD), F32),
            pltpu.VMEM((2, HD, HD), BF16),
            pltpu.VMEM((2, HD, HD), BF16),
            pltpu.VMEM((HD, D), BF16),
            pltpu.VMEM((HD, D), BF16),
            pltpu.VMEM((CHUNKS, NZ, ROWS, WIDE), F32),
            pltpu.VMEM((slots, ROWS, WIDE), BF16),
            pltpu.VMEM((slots, ROWS, WIDE), BF16),
            dma((6,)),
            dma((2,)),
            dma((2,)),
            dma((2 * NZ,)),
            dma((2 * NZ,)),
            dma((NZ,)),
            dma((NZ,)),
            dma((1,)),
            dma((4 * NZ,)),
            dma((1,)),
            dma((4,)),
            dma((3,)),
            dma((NZ + 2,)),
            dma((2,)),
            dma((NZ + 1,)),
            dma((1,)),
            dma((1,)),
            dma((4,)),
            dma((4,)),
            dma((1,)),
            dma((2,)),
            dma((2,)),
            dma((slots,)),
            dma((slots,)),
        ],
        compiler_params=pltpu.CompilerParams(
            collective_id=0, has_side_effects=True, vmem_limit_bytes=60 * 2**20
        ),
        name="whole",
    )(*arrays)


def shards(
    latent, context, condition, context_condition, modulation,
    query_weight, key_weight, value_weight, lambdas, context_lift, head_gain, output_weight,
):
    return run(
        latent, context, condition.reshape(32, 128), context_condition.reshape(32, 128),
        modulation, query_weight, key_weight, value_weight, *[jnp.asarray(t) for t in tables()],
        context_lift, lambdas, head_gain.reshape(1, HD), output_weight,
    )


def solution(mesh):
    split = Mesh(mesh.devices.reshape(4, 4, NZ, 2), ("y", "x", "z", "c"))
    sp, tp = ("y", "x"), ("z", "c")
    return jax.shard_map(
        shards,
        mesh=split,
        in_specs=(
            P(sp + tp, None),
            P(sp, None),
            P(),
            P(),
            P(None, sp, tp),
            P(None, tp),
            P(None, tp),
            P(None, tp),
            P(tp),
            P(tp),
            P(),
            P(tp, None),
        ),
        out_specs=P(sp + tp, None),
        check_vma=False,
    )
```
